32 devices in a mesh: sp: 4 (over z), fs: 4 (over y, x), tp: 2 (over core).
Axes of the slice: x: 2, y: 2, z: 4, core: 2. Of those that a mesh axis runs over, the one named last changes fastest.
Arguments:
- tokens: bfloat16 [4, 640, 2048], P('fs', 'sp', 'tp'), may hold values from -6 to 6
- mix_gain: float32 [2048], replicated, may hold values from 0.1 to 1.9
- conv_b_weight: bfloat16 [2048, 1024], P(('sp', 'fs'), 'tp'), may hold values from -0.125 to 0.125
- conv_c_weight: bfloat16 [2048, 1024], P(('sp', 'fs'), 'tp'), may hold values from -0.125 to 0.125
- conv_v_weight: bfloat16 [2048, 1024], P(('sp', 'fs'), 'tp'), may hold values from -0.125 to 0.125
- conv_taps: float32 [3, 1024], P(None, 'tp'), may hold values from -3.5 to 3.5
- query_weight: bfloat16 [2048, 2048], P(('sp', 'fs'), 'tp'), may hold values from -0.125 to 0.125
- query_rope_weight: bfloat16 [2048, 1024], P(('sp', 'fs'), 'tp'), may hold values from -4.5 to 4.5
- latent_weight: bfloat16 [2048, 512], P(('sp', 'fs')), may hold values from -0.125 to 0.125
- key_rope_weight: bfloat16 [2048, 64], replicated, may hold values from -1 to 1
- latent_gain: float32 [512], replicated, may hold values from 0.1 to 1.9
- key_up_weight: bfloat16 [512, 2048], P(None, 'tp'), may hold values from -0.25 to 0.25
- value_up_weight: bfloat16 [512, 2048], P(None, 'tp'), may hold values from -0.25 to 0.25
- head_gain: float32 [2048], P('tp'), may hold values from 0.1 to 1.9
- conv_out_weight: bfloat16 [1024, 2048], P('tp', ('sp', 'fs')), may hold values from -0.109375 to 0.109375
- attn_out_weight: bfloat16 [2048, 2048], P('tp', ('sp', 'fs')), may hold values from -0.109375 to 0.109375
Outputs:
- mixed: bfloat16 [4, 640, 2048], P('fs', ('sp', 'tp'))
The draws below stay inside these ranges and needn't reach their ends.
All inputs are finite; a program needn't handle non-finite values.
Results may differ from the reference program's by a relative error of at most 0.025.
Values may be sent and summed in bfloat16 or wider, within the bound.
A program may use at most 128 MiB of HBM per device.

```python
import math
import jax
import jax.numpy as jnp
from jax import lax

D = 2048
CONV = 1024
H = 16
NOPE = 128
ROPE = 64
VD = 128
KVL = 512
SEG = 64
SEQS = 4
LENGTH = 640
N_TP = 2


def rope_base(key):
    base = jax.random.normal(jax.random.fold_in(key, 101), (D, ROPE), jnp.float32)
    return jnp.clip(base, -4.0, 4.0) * D ** (-0.5)


def draw_key_rope_weight(key, part):
    return rope_base(key).astype(jnp.bfloat16)


def draw_query_rope_weight(key, part):
    fresh = jax.random.normal(jax.random.fold_in(key, 102), (D, H, ROPE), jnp.float32)
    fresh = jnp.clip(fresh, -4.0, 4.0) * D ** (-0.5)
    shaped = fresh
    return shaped.reshape(D, H * ROPE).astype(jnp.bfloat16)


def block_levels(rng, dims, split, least, high):
    loudness = 1.0
    for dim, parts in split:
        heights = jax.random.uniform(jax.random.fold_in(jax.random.fold_in(rng, 6), dim), (parts,), jnp.float32, least / len(split), high / len(split))
        loudness = loudness * jnp.repeat(jnp.exp(heights), dims[dim] // parts).reshape((-1,) + (1,) * (len(dims) - 1 - dim))
    return loudness


def bell_draw(stream_key, dims, width, bound, shards=(), kind=jnp.bfloat16):
    values = width * jax.random.normal(stream_key, dims, jnp.float32)
    if shards:
        values = values * block_levels(stream_key, dims, shards, -0.22, 0.18)
    return jnp.clip(values, -bound, bound).astype(kind)


def setup_inputs(seed: int = 0) -> dict:
    seeds = jax.random.split(jax.random.key(seed), 17)
    return {
        "tokens": bell_draw(seeds[0], (SEQS, LENGTH, D), 1.0, 6.0, ((0, 4), (1, 4), (2, 2))),
        "mix_gain": jnp.clip(1.0 + 0.18 * jax.random.normal(seeds[1], (D,), jnp.float32), 0.1, 1.9),
        "conv_b_weight": bell_draw(seeds[2], (D, CONV), D ** -0.5, 0.125, ((0, 16), (1, 2))),
        "conv_c_weight": bell_draw(seeds[3], (D, CONV), D ** -0.5, 0.125, ((0, 16), (1, 2))),
        "conv_v_weight": bell_draw(seeds[4], (D, CONV), D ** -0.5, 0.125, ((0, 16), (1, 2))),
        "conv_taps": bell_draw(seeds[5], (3, CONV), 3 ** -0.5, 3.5, ((1, 2),), jnp.float32),
        "query_weight": bell_draw(seeds[6], (D, H * NOPE), D ** -0.5, 0.125, ((0, 16), (1, 2))),
        "query_rope_weight": draw_query_rope_weight(jax.random.fold_in(seeds[16], 71), 0),
        "latent_weight": bell_draw(seeds[8], (D, KVL), D ** -0.5, 0.125, ((0, 16),)),
        "key_rope_weight": draw_key_rope_weight(jax.random.fold_in(seeds[16], 71), 0),
        "latent_gain": jnp.clip(1.0 + 0.18 * jax.random.normal(seeds[10], (KVL,), jnp.float32), 0.1, 1.9),
        "key_up_weight": bell_draw(seeds[11], (KVL, H * NOPE), KVL ** -0.5, 0.25, ((1, 2),)),
        "value_up_weight": bell_draw(seeds[12], (KVL, H * VD), KVL ** -0.5, 0.25, ((1, 2),)),
        "head_gain": jnp.clip(1.0 + 0.18 * jax.random.normal(seeds[13], (H * VD,), jnp.float32), 0.1, 1.9),
        "conv_out_weight": bell_draw(seeds[14], (CONV, D), (CONV + H * VD) ** -0.5, 0.109375, ((0, 2), (1, 16))),
        "attn_out_weight": bell_draw(seeds[15], (H * VD, D), (CONV + H * VD) ** -0.5, 0.109375, ((0, 2), (1, 16))),
    }


norm_epsilon = 1e-06
rope_theta = 10000.0

def rms_scale(values, gain):
    return values * lax.rsqrt(lax.optimization_barrier(jnp.mean(values * values, axis=-1, keepdims=True)) + norm_epsilon) * gain

def rope_tables(positions):
    half_width = ROPE // 2
    frequency = rope_theta ** (-jnp.arange(half_width, dtype=jnp.float32) * 2.0 / ROPE)
    angles = positions[:, None] * frequency[None, :]
    return (jnp.cos(angles), jnp.sin(angles))

def rotate(values, cosine, sine):
    half_width = ROPE // 2
    first = values[..., :half_width]
    second = values[..., half_width:]
    return jnp.concatenate([first * cosine - second * sine, second * cosine + first * sine], axis=-1)

def matmul(left, right):
    return jnp.dot(left, right, preferred_element_type=jnp.float32)

def one_sequence(sequence, mix_gain, conv_b_weight, conv_c_weight, conv_v_weight, conv_taps, query_weight, query_rope_weight, latent_weight, key_rope_weight, latent_gain, key_up_weight, value_up_weight, head_gain, conv_out_weight, attn_out_weight):
    length = sequence.shape[0]
    normed = rms_scale(sequence.astype(jnp.float32), mix_gain).astype(jnp.bfloat16)
    gate_b = matmul(normed, conv_b_weight).astype(jnp.bfloat16)
    gate_c = matmul(normed, conv_c_weight).astype(jnp.bfloat16)
    values_v = matmul(normed, conv_v_weight).astype(jnp.bfloat16)
    product = (gate_c.astype(jnp.float32) * values_v.astype(jnp.float32)).astype(jnp.bfloat16)
    padded = jnp.concatenate([jnp.zeros((2, CONV), jnp.bfloat16), product], axis=0).astype(jnp.float32)
    convolved = conv_taps[0] * padded[0:length] + conv_taps[1] * padded[1:length + 1] + conv_taps[2] * padded[2:length + 2]
    conv_y = (gate_b.astype(jnp.float32) * convolved).astype(jnp.bfloat16)
    positions = jnp.arange(length, dtype=jnp.float32)
    cosine, sine = rope_tables(positions)
    query_nope = matmul(normed, query_weight).astype(jnp.bfloat16).reshape(length, H, NOPE)
    query_rot = rotate(matmul(normed, query_rope_weight).reshape(length, H, ROPE), cosine[:, None, :], sine[:, None, :]).astype(jnp.bfloat16)
    latent_raw = matmul(normed, latent_weight).astype(jnp.bfloat16)
    latent = rms_scale(latent_raw.astype(jnp.float32), latent_gain).astype(jnp.bfloat16)
    key_rot = rotate(matmul(normed, key_rope_weight), cosine, sine).astype(jnp.bfloat16)
    query_latent = jnp.einsum('thn,khn->thk', query_nope.astype(jnp.float32), key_up_weight.reshape(KVL, H, NOPE).astype(jnp.float32)).astype(jnp.bfloat16)
    attn_scale = (NOPE + ROPE) ** (-0.5)
    block_rows = math.gcd(length, 512)
    latent_wide = latent.astype(jnp.float32)
    key_wide = key_rot.astype(jnp.float32)
    key_segment = jnp.arange(length, dtype=jnp.int32) // SEG

    def attend(block_index):
        begin_row = (block_index * block_rows).astype(jnp.int32)
        block_latent = lax.dynamic_slice_in_dim(query_latent, begin_row, block_rows, 0).astype(jnp.float32)
        block_rot = lax.dynamic_slice_in_dim(query_rot, begin_row, block_rows, 0).astype(jnp.float32)
        scores = (jnp.einsum('thk,jk->thj', block_latent, latent_wide) + jnp.einsum('thr,jr->thj', block_rot, key_wide)) * attn_scale
        query_segment = (begin_row + jnp.arange(block_rows, dtype=jnp.int32)) // SEG
        allowed = key_segment[None, None, :] <= query_segment[:, None, None]
        scores = jnp.where(allowed, scores, -1e+30)
        highest = lax.optimization_barrier(jnp.max(scores, axis=-1, keepdims=True))
        weights = jnp.where(allowed, jnp.exp(scores - highest), 0.0)
        summed = lax.optimization_barrier(jnp.sum(weights, axis=-1))
        numer = jnp.einsum('thj,jk->thk', weights.astype(jnp.bfloat16).astype(jnp.float32), latent_wide)
        return (numer / summed[..., None]).astype(jnp.bfloat16)
    attended = lax.map(attend, jnp.arange(length // block_rows, dtype=jnp.int32)).reshape(length, H, KVL)
    head_out = jnp.einsum('thk,khv->thv', attended.astype(jnp.float32), value_up_weight.reshape(KVL, H, VD).astype(jnp.float32))
    attn_y = rms_scale(head_out, head_gain.reshape(H, VD)).astype(jnp.bfloat16).reshape(length, H * VD)
    conv_share = CONV // N_TP
    head_share = H * VD // N_TP
    combined = jnp.zeros((length, D), jnp.float32)
    for share in range(N_TP):
        conv_cols = slice(share * conv_share, (share + 1) * conv_share)
        head_cols = slice(share * head_share, (share + 1) * head_share)
        partial_out = matmul(conv_y[:, conv_cols], conv_out_weight[conv_cols]) + matmul(attn_y[:, head_cols], attn_out_weight[head_cols])
        rounded = lax.optimization_barrier(partial_out.astype(jnp.bfloat16))
        combined = combined + rounded.astype(jnp.float32)
    return combined.astype(jnp.bfloat16)

def reference(tokens, mix_gain, conv_b_weight, conv_c_weight, conv_v_weight, conv_taps, query_weight, query_rope_weight, latent_weight, key_rope_weight, latent_gain, key_up_weight, value_up_weight, head_gain, conv_out_weight, attn_out_weight):
    results = []
    for sequence_index in range(SEQS):
        results.append(one_sequence(tokens[sequence_index], mix_gain, conv_b_weight, conv_c_weight, conv_v_weight, conv_taps, query_weight, query_rope_weight, latent_weight, key_rope_weight, latent_gain, key_up_weight, value_up_weight, head_gain, conv_out_weight, attn_out_weight))
    return jnp.stack(results, axis=0)
```

```python
import functools

import jax
import jax.numpy as jnp
from jax import lax
from jax.experimental import pallas as pl
from jax.experimental.pallas import tpu as pltpu
from jax.sharding import PartitionSpec as P

NOPE = 128
ROPE = 64
VD = 128
KVL = 512
SEG = 64


norm_epsilon = 1e-06
rope_theta = 10000.0


def passed_along(block, axis, distance):
    devices = range(lax.axis_size(axis))
    route = [(i - distance, i) for i in devices if i - distance in devices]
    return lax.ppermute(block, axis, route)


def rms_scale(values, gain):
    return (
        values * lax.rsqrt(jnp.mean(values * values, axis=-1, keepdims=True) + norm_epsilon) * gain
    )


def rope_tables(positions):
    half_width = ROPE // 2
    frequency = rope_theta ** (-jnp.arange(half_width, dtype=jnp.float32) * 2.0 / ROPE)
    angles = positions[:, None] * frequency[None, :]
    return (jnp.cos(angles), jnp.sin(angles))


def rotate(values, cosine, sine):
    half_width = ROPE // 2
    first = values[..., :half_width]
    second = values[..., half_width:]
    return jnp.concatenate(
        [first * cosine - second * sine, second * cosine + first * sine], axis=-1
    )


def general_shards(
    tokens,
    mix_gain,
    conv_b_weight,
    conv_c_weight,
    conv_v_weight,
    conv_taps,
    query_weight,
    query_rope_weight,
    latent_weight,
    key_rope_weight,
    latent_gain,
    key_up_weight,
    value_up_weight,
    head_gain,
    conv_out_weight,
    attn_out_weight,
):
    full_rows = lax.all_gather(tokens[0], "tp", axis=1, tiled=True)
    tok_rows = full_rows.shape[0]
    normed = rms_scale(full_rows.astype(jnp.float32), mix_gain).astype(jnp.bfloat16)
    offset = lax.axis_index("sp") * tok_rows
    token_index = offset + jnp.arange(tok_rows, dtype=jnp.int32)
    cosine, sine = rope_tables(token_index.astype(jnp.float32))
    local_heads = query_weight.shape[1] // NOPE
    count_sp = lax.axis_size("sp")
    count_fs = lax.axis_size("fs")
    count_tp = lax.axis_size("tp")
    fs_index = lax.axis_index("fs")
    row_piece = normed.shape[1] // (count_sp * count_fs)
    all_normed = lax.all_gather(normed, "fs", axis=0, tiled=True)
    picked = lax.dynamic_index_in_dim(
        all_normed.reshape(-1, count_sp, count_fs, row_piece), fs_index, 2, keepdims=False
    ).reshape(-1, count_sp * row_piece)
    gathered = (
        lax.all_gather(conv_b_weight, "sp", axis=0, tiled=True),
        lax.all_gather(conv_c_weight, "sp", axis=0, tiled=True),
        lax.all_gather(conv_v_weight, "sp", axis=0, tiled=True),
        lax.all_gather(query_weight, "sp", axis=0, tiled=True),
        lax.all_gather(query_rope_weight, "sp", axis=0, tiled=True),
        lax.all_gather(latent_weight, "sp", axis=0, tiled=True),
    )

    def project_in():
        return jnp.concatenate(
            [jnp.dot(picked, member, preferred_element_type=jnp.float32) for member in gathered],
            axis=1,
        )

    joined = lax.psum_scatter(
        project_in().astype(jnp.bfloat16), "fs", scatter_dimension=0, tiled=True
    ).astype(jnp.float32)
    bounds = []
    running_total = 0
    for member in gathered[:-1]:
        running_total = running_total + member.shape[1]
        bounds.append(running_total)
    sums = tuple(jnp.split(joined, bounds, axis=1))
    latent_raw = sums[5].astype(jnp.bfloat16)
    gate_b = sums[0].astype(jnp.bfloat16)
    gate_c = sums[1].astype(jnp.bfloat16)
    values_v = sums[2].astype(jnp.bfloat16)
    query_nope = sums[3].astype(jnp.bfloat16).reshape(tok_rows, local_heads, NOPE)
    query_rot = rotate(
        sums[4].reshape(tok_rows, local_heads, ROPE), cosine[:, None, :], sine[:, None, :]
    ).astype(jnp.bfloat16)
    latent = rms_scale(latent_raw.astype(jnp.float32), latent_gain).astype(jnp.bfloat16)
    key_rot = rotate(
        jnp.dot(normed, key_rope_weight, preferred_element_type=jnp.float32), cosine, sine
    ).astype(jnp.bfloat16)
    query_latent = jnp.einsum(
        "thn,khn->thk",
        query_nope,
        key_up_weight.reshape(KVL, local_heads, NOPE),
        preferred_element_type=jnp.float32,
    ).astype(jnp.bfloat16)
    attn_scale = (NOPE + ROPE) ** (-0.5)
    product = (gate_c.astype(jnp.float32) * values_v.astype(jnp.float32)).astype(jnp.bfloat16)
    previous = passed_along(product[tok_rows - 2 :], "sp", 1)
    padded = jnp.concatenate([previous, product], axis=0).astype(jnp.float32)
    convolved = (
        conv_taps[0] * padded[0:tok_rows]
        + conv_taps[1] * padded[1 : tok_rows + 1]
        + conv_taps[2] * padded[2 : tok_rows + 2]
    )
    conv_y = (gate_b.astype(jnp.float32) * convolved).astype(jnp.bfloat16)
    query_segment = token_index // SEG
    last_segment = (offset + tok_rows - 1) // SEG

    def key_block(running, latent_block, rot_block, first_key):
        peak_old, denom_old, accum_old = running
        block_rows = latent_block.shape[0]
        scores = (
            jnp.einsum(
                "thk,jk->thj", query_latent, latent_block, preferred_element_type=jnp.float32
            )
            + jnp.einsum("thr,jr->thj", query_rot, rot_block, preferred_element_type=jnp.float32)
        ) * attn_scale
        key_segment = (first_key + jnp.arange(block_rows, dtype=jnp.int32)) // SEG
        allowed = key_segment[None, None, :] <= query_segment[:, None, None]
        peak_new = jnp.maximum(peak_old, jnp.max(jnp.where(allowed, scores, -1e30), axis=-1))
        weights = jnp.where(allowed, jnp.exp(scores - peak_new[..., None]), 0.0)
        rescale = jnp.exp(peak_old - peak_new)
        denom_new = denom_old * rescale + jnp.sum(weights, axis=-1)
        accum_new = accum_old * rescale[..., None] + jnp.einsum(
            "thj,jk->thk",
            weights.astype(jnp.bfloat16),
            latent_block,
            preferred_element_type=jnp.float32,
        )
        return (peak_new, denom_new, accum_new)

    starting = (
        jnp.full((tok_rows, local_heads), -1e30, jnp.float32),
        jnp.zeros((tok_rows, local_heads), jnp.float32),
        jnp.zeros((tok_rows, local_heads, KVL), jnp.float32),
    )
    latent_piece = lax.all_gather(latent, "sp", axis=0, tiled=True)
    rot_piece = lax.all_gather(key_rot, "sp", axis=0, tiled=True)
    piece_rows = latent_piece.shape[0]
    splits = max(1, piece_rows // 512)
    while piece_rows % splits:
        splits = splits - 1
    block_rows = piece_rows // splits

    def visit(state, block_index):
        block_begin = block_index * block_rows
        latent_block = lax.dynamic_slice_in_dim(latent_piece, block_begin, block_rows, 0)
        rot_block = lax.dynamic_slice_in_dim(rot_piece, block_begin, block_rows, 0)
        updated = lax.cond(
            block_begin // SEG <= last_segment,
            lambda inner: key_block(inner, latent_block, rot_block, block_begin),
            lambda inner: inner,
            state,
        )
        return (updated, None)

    peak, denom, accum = lax.scan(visit, starting, jnp.arange(splits, dtype=jnp.int32))[0]
    attended = (accum / denom[..., None]).astype(jnp.bfloat16)
    head_out = jnp.einsum(
        "thk,khv->thv",
        attended,
        value_up_weight.reshape(KVL, local_heads, VD),
        preferred_element_type=jnp.float32,
    )
    normed_heads = rms_scale(head_out, head_gain.reshape(local_heads, VD))
    attn_y = normed_heads.astype(jnp.bfloat16).reshape(tok_rows, local_heads * VD)
    share_rows = tok_rows // count_tp
    conv_all, attn_all = (
        lax.all_gather(conv_y, "fs", axis=0, tiled=True),
        lax.all_gather(attn_y, "fs", axis=0, tiled=True),
    )
    conv_sorted = (
        conv_all.reshape(count_fs, count_tp, share_rows, -1)
        .transpose(1, 0, 2, 3)
        .reshape(count_fs * tok_rows, -1)
    )
    attn_sorted = (
        attn_all.reshape(count_fs, count_tp, share_rows, -1)
        .transpose(1, 0, 2, 3)
        .reshape(count_fs * tok_rows, -1)
    )
    conv_cols_sp, attn_cols_sp = (
        lax.all_gather(conv_out_weight, "sp", axis=1, tiled=True),
        lax.all_gather(attn_out_weight, "sp", axis=1, tiled=True),
    )
    col_sums = lax.psum_scatter(
        (
            jnp.dot(conv_sorted, conv_cols_sp, preferred_element_type=jnp.float32)
            + jnp.dot(attn_sorted, attn_cols_sp, preferred_element_type=jnp.float32)
        ).astype(jnp.bfloat16),
        "tp",
        scatter_dimension=0,
        tiled=True,
    )
    col_piece = conv_cols_sp.shape[1] // count_sp
    outgoing = col_sums.reshape(count_fs, share_rows, count_sp * col_piece)
    arrived = lax.all_to_all(outgoing, "fs", split_axis=0, concat_axis=2, tiled=True)
    result = (
        arrived.reshape(share_rows, count_fs, count_sp, col_piece)
        .transpose(0, 2, 1, 3)
        .reshape(share_rows, count_fs * count_sp * col_piece)
    )
    return result[None]


MESH = pl.DeviceIdType.MESH


class Place:
    def __init__(self):
        self.z = lax.axis_index("sp")
        self.f = lax.axis_index("fs")
        self.c = lax.axis_index("tp")

    def to(self, z=None, f=None, c=None):
        return {
            "sp": self.z if z is None else z,
            "fs": self.f if f is None else f,
            "tp": self.c if c is None else c,
        }


def flip(index, bit):
    digit = (index // bit) % 2
    return index + bit * (1 - 2 * digit)


def remote(src, dst, send, recv, device):
    return pltpu.make_async_remote_copy(
        src_ref=src, dst_ref=dst, send_sem=send, recv_sem=recv, device_id=device, device_id_type=MESH
    )


def greet(devices):
    barrier = pltpu.get_barrier_semaphore()
    for device in devices:
        pl.semaphore_signal(barrier, inc=1, device_id=device, device_id_type=MESH)
    pl.semaphore_wait(barrier, len(devices))


def gather_kernel(
    n,
    tok_in,
    gain,
    cb,
    cc,
    cv,
    qw,
    qr,
    lw,
    krw,
    co,
    ao,
    proj_out,
    lat_out,
    krot_out,
    wout,
    tok,
    normed,
    win,
    lat,
    wsem,
    lsem,
    tsem,
    psem,
    latsem,
):
    here = Place()
    z, f, c = here.z, here.f, here.c
    fx, fy = flip(f, 1), flip(f, 2)
    other = 1 - c
    rows = cb.shape[0]
    members = (cb, cc, cv, qw, qr, lw)
    widths = [m.shape[1] // n for m in members]
    starts = [sum(widths[:i]) for i in range(len(widths))]
    total = sum(widths)
    lat_w = widths[-1]
    proj_w = total - lat_w
    tr = tok_in.shape[1]
    length = n * tr
    half = length // 2
    outs = (co, ao)
    heights = [m.shape[0] // n for m in outs]
    tops = [sum(heights[:i]) for i in range(len(heights))]
    out_cols = co.shape[1]

    steps = [(1 + j, s) for j in range(n - 1) for s in (-1, 1)]

    greet(
        [here.to(z=lax.rem(z + j, n)) for j in range(1, n)]
        + [here.to(f=fx), here.to(f=fy), here.to(c=other)]
    )

    def in_block(zs, fs):
        return win.at[pl.ds(pl.multiple_of((zs * 4 + fs) * rows, rows), rows), :]

    def out_block(zs, fs):
        return wout.at[:, pl.ds(pl.multiple_of((zs * 4 + fs) * out_cols, out_cols), out_cols)]

    blocks = (in_block, out_block)

    def pieces(kind, dest):
        found = []
        if kind == 0:
            dst = (z * 4 + f) * rows
            for m, w, s in zip(members, widths, starts):
                src = m.at[:, pl.ds(pl.multiple_of(dest * w, w), w)]
                found.append((src, win.at[pl.ds(pl.multiple_of(dst, rows), rows), pl.ds(s, w)]))
        else:
            dst = (z * 4 + f) * out_cols
            for m, h, s in zip(outs, heights, tops):
                src = m.at[pl.ds(pl.multiple_of(dest * h, h), h), :]
                found.append((src, wout.at[pl.ds(s, h), pl.ds(pl.multiple_of(dst, out_cols), out_cols)]))
        return found

    def send_own(kind):
        for src, dst in pieces(kind, z):
            remote(src, dst, wsem.at[kind, 2, z], wsem.at[kind, 3, z], here.to(f=fx)).start()
            remote(src, dst, wsem.at[kind, 4, z], wsem.at[kind, 5, z], here.to(f=fy)).start()
            pltpu.make_async_copy(src, dst, lsem.at[kind]).start()

    def send_z(kind, distance, sign):
        dest = z + sign * distance

        @pl.when((dest >= 0) & (dest < n))
        def _():
            for src, dst in pieces(kind, dest):
                remote(src, dst, wsem.at[kind, 0, dest], wsem.at[kind, 1, z], here.to(z=dest)).start()

    def plane_copy(kind, zs, role, fs, to):
        block = blocks[kind](zs, fs)
        return remote(block, block, wsem.at[kind, role, zs], wsem.at[kind, role + 1, zs], here.to(f=to))

    def relay_z(kind, distance, sign):
        zs = z + sign * distance

        @pl.when((zs >= 0) & (zs < n))
        def _():
            block = blocks[kind](zs, f)
            remote(block, block, wsem.at[kind, 0, zs], wsem.at[kind, 1, zs], here.to(z=zs)).wait_recv()
            plane_copy(kind, zs, 2, f, fx).start()
            plane_copy(kind, zs, 4, f, fy).start()

    def relay_plane(kind, zs):
        plane_copy(kind, zs, 2, fx, fx).wait_recv()

        @pl.when(zs % 2 == 0)
        def _():
            plane_copy(kind, zs, 6, fx, fy).start()

        plane_copy(kind, zs, 4, fy, fy).wait_recv()

        @pl.when(zs % 2 == 1)
        def _():
            plane_copy(kind, zs, 6, fy, fx).start()

    def tok_block(half_index, zs):
        return tok.at[half_index, pl.ds(pl.multiple_of(zs * tr, tr), tr), :]

    def tok_copy(zs, sign, hop, src=None):
        d = (sign + 1) // 2
        block = tok_block(c, zs)
        return remote(
            block if src is None else src, block, tsem.at[d, 0, hop], tsem.at[d, 1, hop], here.to(z=z + sign)
        )

    def partner_copy(zs, owner, src=None):
        block = tok_block(owner, zs)
        return remote(block if src is None else src, block, psem.at[0, zs], psem.at[1, zs], here.to(c=other))

    own_tok = tok_in.at[0]

    def can(sign):
        return (z + sign >= 0) & (z + sign < n)

    send_own(0)
    for distance, sign in steps[:2]:
        send_z(0, distance, sign)
    partner_copy(z, c, own_tok).start()
    pltpu.make_async_copy(own_tok, tok_block(c, z), lsem.at[2]).start()
    for sign in (-1, 1):
        pl.when(can(sign))(lambda sign=sign: tok_copy(z, sign, 0, own_tok).start())
    for distance, sign in steps[2:]:
        send_z(0, distance, sign)

    def relay_tok(distance, sign):
        zs = z + sign * distance

        @pl.when((zs >= 0) & (zs < n))
        def _():
            tok_copy(zs, -sign, distance - 1).wait_recv()
            if distance < n - 1:
                pl.when(can(-sign))(lambda: tok_copy(zs, -sign, distance).start())
            partner_copy(zs, c).start()

    for distance, sign in steps:
        relay_z(0, distance, sign)
        relay_tok(distance, sign)
    send_own(1)
    for distance, sign in steps:
        send_z(1, distance, sign)

    def each_zs(fn):
        def body(i, carry):
            fn(lax.rem(z + i, n))
            return carry

        lax.fori_loop(0, n, body, 0)

    def tok_ready(zs):
        partner_copy(zs, other).wait_recv()

    each_zs(tok_ready)
    pltpu.make_async_copy(own_tok, tok_block(c, z), lsem.at[2]).wait()
    chunk = tr // 2
    wide = tok.shape[2]

    def norm_chunk(i, carry):
        at = pl.ds(pl.multiple_of(i * chunk, chunk), chunk)
        first = tok[0, at, :].astype(jnp.float32)
        second = tok[1, at, :].astype(jnp.float32)
        mean = (
            jnp.sum(first * first, axis=-1, keepdims=True) + jnp.sum(second * second, axis=-1, keepdims=True)
        ) / (2 * wide)
        scale = lax.rsqrt(mean + norm_epsilon)
        normed[at, 0:wide] = (first * scale * gain[0, :]).astype(jnp.bfloat16)
        normed[at, wide : 2 * wide] = (second * scale * gain[1, :]).astype(jnp.bfloat16)
        return carry

    each_zs(lambda zs: relay_plane(0, zs))
    lax.fori_loop(0, 2 * n, norm_chunk, 0)
    for distance, sign in steps:
        relay_z(1, distance, sign)

    def relay_done(kind, zs):
        plane_copy(kind, zs, 6, flip(fx, 2), fx).wait_recv()

    for src, dst in pieces(0, z)[:1]:
        pltpu.make_async_copy(in_block(z, f), in_block(z, f), lsem.at[0]).wait()
    each_zs(lambda zs: relay_done(0, zs))

    def lat_block(zs, owner):
        return lat.at[zs, pl.ds(pl.multiple_of(owner * half, half), half), :]

    def lat_copy(dest):
        return remote(lat_block(z, c), lat_block(z, c), latsem.at[0, dest], latsem.at[1, z], here.to(z=dest))

    def lat_arrival(zs):
        return remote(lat_block(zs, c), lat_block(zs, c), latsem.at[0, zs], latsem.at[1, zs], here.to(z=zs))

    def lat_partner(zs, owner):
        return remote(
            lat_block(zs, owner), lat_block(zs, owner), latsem.at[2, zs], latsem.at[3, zs], here.to(c=other)
        )

    mine = pl.ds(pl.multiple_of(c * half, half), half)
    lat[z, mine, :] = jnp.dot(
        normed[mine, :], win[:, proj_w:total], preferred_element_type=jnp.float32
    ).astype(jnp.bfloat16)
    for j in range(1, n):
        lat_copy(lax.rem(z + j, n)).start()
    lat_partner(z, c).start()
    each_zs(lambda zs: relay_plane(1, zs))

    def project(i, carry):
        at = pl.ds(pl.multiple_of(i * tr, tr), tr)
        proj_out[at, :] = jnp.dot(
            normed[at, :], win[:, 0:proj_w], preferred_element_type=jnp.float32
        ).astype(jnp.bfloat16)
        krot_out[at, :] = jnp.dot(normed[at, :], krw[...], preferred_element_type=jnp.float32)
        return carry

    lax.fori_loop(0, n, project, 0)
    for j in range(1, n):
        zs = lax.rem(z + j, n)
        lat_arrival(zs).wait_recv()
        lat_partner(zs, c).start()
    each_zs(lambda zs: lat_partner(zs, other).wait_recv())
    for k in range(n):
        lat_out[:, k * lat_w : (k + 1) * lat_w] = lat[k]

    pltpu.make_async_copy(out_block(z, f), out_block(z, f), lsem.at[1]).wait()
    each_zs(lambda zs: relay_done(1, zs))
    for j in range(1, n):
        zs = lax.rem(z + j, n)
        for kind in (0, 1):
            block = blocks[kind](zs, f)
            remote(block, block, wsem.at[kind, 0, zs], wsem.at[kind, 1, zs], here.to(z=zs)).wait_send()
        lat_copy(zs).wait_send()

    def sent(zs):
        for kind in (0, 1):
            plane_copy(kind, zs, 2, f, fx).wait_send()
            plane_copy(kind, zs, 4, f, fy).wait_send()
            plane_copy(kind, zs, 6, fx, fy).wait_send()
        partner_copy(zs, c).wait_send()
        lat_partner(zs, c).wait_send()

    each_zs(sent)
    for sign in (-1, 1):
        pl.when(can(sign))(lambda sign=sign: tok_copy(z, sign, 0).wait_send())
        for distance in range(1, n - 1):
            zs = z - sign * distance
            pl.when((zs >= 0) & (zs < n) & can(sign))(
                lambda sign=sign, distance=distance: tok_copy(z, sign, distance).wait_send()
            )


def reduce_kernel(n, part, out, own, pair, moving, fetched, csem, psem, zsem):
    here = Place()
    z, c = here.z, here.c
    other = 1 - c
    share = out.shape[0]
    greet(
        [here.to(c=other)]
        + [here.to(z=lax.rem(z + 1, n)), here.to(z=lax.rem(z + n - 1, n))]
    )

    def rows(zs, core):
        return part.at[pl.ds(pl.multiple_of((2 * zs + core) * share, share), share), :]

    def pair_copy(zs):
        return remote(rows(zs, other), pair.at[zs], psem.at[0, zs], psem.at[1, zs], here.to(c=other))

    def own_copy(zs):
        return pltpu.make_async_copy(rows(zs, c), own.at[zs], csem.at[zs])

    order = [j for j in range(n - 1, -1, -1)]

    def line_copy(d, dest):
        return remote(
            moving.at[d, dest],
            fetched.at[d, dest],
            zsem.at[d, 0, dest],
            zsem.at[d, 1, dest],
            here.to(z=z + 2 * d - 1),
        )

    turns = [(far, d) for far in range(n - 1, -1, -1) for d in (0, 1)]
    for far, d in turns:
        dest = z + (2 * d - 1) * far
        if far == 0 and d == 1:
            continue

        @pl.when((dest >= 0) & (dest < n))
        def _():
            pair_copy(dest).start()
            own_copy(dest).start()

    def summed(dest):
        return own[dest].astype(jnp.float32) + pair[dest].astype(jnp.float32)

    for far, d in turns:
        dest = z + (2 * d - 1) * far
        if far == 0:
            continue

        @pl.when((dest >= 0) & (dest < n))
        def _():
            own_copy(dest).wait()
            pair_copy(dest).wait_recv()
            before = z - (2 * d - 1)
            has = (before >= 0) & (before < n)

            @pl.when(has)
            def _():
                line_copy(d, dest).wait_recv()
                moving[d, dest] = (summed(dest) + fetched[d, dest].astype(jnp.float32)).astype(jnp.bfloat16)

            @pl.when(jnp.logical_not(has))
            def _():
                moving[d, dest] = summed(dest).astype(jnp.bfloat16)

            line_copy(d, dest).start()

    own_copy(z).wait()
    pair_copy(z).wait_recv()
    low, high = z > 0, z < n - 1

    @pl.when(low)
    def _():
        line_copy(1, z).wait_recv()

    @pl.when(high)
    def _():
        line_copy(0, z).wait_recv()

    result = summed(z)
    from_low = fetched[1, z].astype(jnp.float32)
    from_high = fetched[0, z].astype(jnp.float32)
    zero = jnp.zeros_like(result)
    result = result + jnp.where(low, from_low, zero) + jnp.where(high, from_high, zero)
    out[...] = result.astype(jnp.bfloat16)

    for far, d in turns:
        dest = z + (2 * d - 1) * far
        if far == 0 and d == 1:
            continue

        @pl.when((dest >= 0) & (dest < n))
        def _():
            pair_copy(dest).wait_send()
            if far:
                line_copy(d, dest).wait_send()


def split_shards(
    tokens,
    mix_gain,
    conv_b_weight,
    conv_c_weight,
    conv_v_weight,
    conv_taps,
    query_weight,
    query_rope_weight,
    latent_weight,
    key_rope_weight,
    latent_gain,
    key_up_weight,
    value_up_weight,
    head_gain,
    conv_out_weight,
    attn_out_weight,
):
    n = lax.axis_size("sp")
    z = lax.axis_index("sp")
    tr = tokens.shape[1]
    wide = tokens.shape[2]
    length = n * tr
    features = 2 * wide
    heads = query_weight.shape[1] // NOPE // n
    channels = conv_b_weight.shape[1] // n
    lat_w = latent_weight.shape[1] // n
    proj_w = 3 * channels + heads * (NOPE + ROPE)
    out_rows = (conv_out_weight.shape[0] + attn_out_weight.shape[0]) // n
    columns = attn_out_weight.shape[1] * n * 4
    bf16 = jnp.bfloat16
    vmem = pl.BlockSpec(memory_space=pltpu.VMEM)
    anywhere = pl.BlockSpec(memory_space=pl.ANY)
    dma = pltpu.SemaphoreType.DMA
    proj, lat_raw, krot_raw, wout = pl.pallas_call(
        functools.partial(gather_kernel, n),
        out_shape=(
            jax.ShapeDtypeStruct((length, proj_w), bf16),
            jax.ShapeDtypeStruct((length, n * lat_w), bf16),
            jax.ShapeDtypeStruct((length, ROPE), jnp.float32),
            jax.ShapeDtypeStruct((out_rows, columns), bf16),
        ),
        in_specs=[anywhere, vmem] + [anywhere] * 6 + [vmem] + [anywhere] * 2,
        out_specs=(vmem, vmem, vmem, anywhere),
        scratch_shapes=[
            pltpu.VMEM((2, length, wide), bf16),
            pltpu.VMEM((length, features), bf16),
            pltpu.VMEM((features, proj_w + lat_w), bf16),
            pltpu.VMEM((n, length, lat_w), bf16),
            dma((2, 8, n)),
            dma((3,)),
            dma((2, 2, n)),
            dma((2, n)),
            dma((4, n)),
        ],
        compiler_params=pltpu.CompilerParams(
            collective_id=0, has_side_effects=True, vmem_limit_bytes=48 * 1024 * 1024
        ),
        name="gather_project",
    )(
        tokens,
        mix_gain.reshape(2, wide),
        conv_b_weight,
        conv_c_weight,
        conv_v_weight,
        query_weight,
        query_rope_weight,
        latent_weight,
        key_rope_weight,
        conv_out_weight,
        attn_out_weight,
    )
    f32 = jnp.float32

    def mine(array, axis):
        width = array.shape[axis] // n
        return lax.dynamic_slice_in_dim(array, z * width, width, axis)

    taps = mine(conv_taps, 1)
    key_up = mine(key_up_weight, 1)
    value_up = mine(value_up_weight, 1)
    gain = mine(head_gain, 0).reshape(heads, VD)
    cosine, sine = rope_tables(jnp.arange(length, dtype=f32))
    gate_b, gate_c, values_v = (proj[:, i * channels : (i + 1) * channels].astype(f32) for i in range(3))
    at = 3 * channels
    query_nope = proj[:, at : at + heads * NOPE].reshape(length, heads, NOPE)
    at = at + heads * NOPE
    query_rot = rotate(
        proj[:, at:].astype(f32).reshape(length, heads, ROPE), cosine[:, None, :], sine[:, None, :]
    ).astype(bf16)
    product = (gate_c * values_v).astype(bf16)
    padded = jnp.concatenate([jnp.zeros((2, channels), bf16), product], axis=0).astype(f32)
    convolved = taps[0] * padded[0:length] + taps[1] * padded[1 : length + 1] + taps[2] * padded[2 : length + 2]
    conv_y = (gate_b * convolved).astype(bf16)
    latent = rms_scale(lat_raw.astype(f32), latent_gain).astype(bf16)
    key_rot = rotate(krot_raw, cosine, sine).astype(bf16)
    keys = jnp.dot(latent, key_up, preferred_element_type=f32).astype(bf16).reshape(length, heads, NOPE)
    values = jnp.dot(latent, value_up, preferred_element_type=f32).astype(bf16).reshape(length, heads, VD)
    scores = (
        jnp.einsum("thn,jhn->htj", query_nope, keys, preferred_element_type=f32)
        + jnp.einsum("thr,jr->htj", query_rot, key_rot, preferred_element_type=f32)
    ) * (NOPE + ROPE) ** (-0.5)
    segment = jnp.arange(length, dtype=jnp.int32) // SEG
    allowed = segment[None, None, :] <= segment[None, :, None]
    scores = jnp.where(allowed, scores, -1e30)
    weights = jnp.exp(scores - jnp.max(scores, axis=-1, keepdims=True))
    denom = jnp.sum(weights, axis=-1)
    head_out = jnp.einsum("htj,jhv->thv", weights.astype(bf16), values, preferred_element_type=f32)
    head_out = head_out / denom.T[:, :, None]
    attn_y = rms_scale(head_out, gain).astype(bf16).reshape(length, heads * VD)
    mixed_y = jnp.concatenate([conv_y, attn_y], axis=1)
    part = jnp.dot(mixed_y, wout, preferred_element_type=f32).astype(bf16)
    share = tr // 2
    result = pl.pallas_call(
        functools.partial(reduce_kernel, n),
        out_shape=jax.ShapeDtypeStruct((share, columns), bf16),
        in_specs=[anywhere],
        out_specs=vmem,
        scratch_shapes=[
            pltpu.VMEM((n, share, columns), bf16),
            pltpu.VMEM((n, share, columns), bf16),
            pltpu.VMEM((2, n, share, columns), bf16),
            pltpu.VMEM((2, n, share, columns), bf16),
            dma((n,)),
            dma((2, n)),
            dma((2, 2, n)),
        ],
        compiler_params=pltpu.CompilerParams(
            collective_id=1, has_side_effects=True, vmem_limit_bytes=32 * 1024 * 1024
        ),
        name="reduce_partials",
    )(part)
    return result[None]


def splits_well(mesh):
    n = mesh.shape["sp"]
    return n > 2 and n <= 4 and mesh.shape["fs"] == 4 and mesh.shape["tp"] == 2


def shards(*arrays):
    n = lax.axis_size("sp")
    conv, query, rope, low_rank = (arrays[i].shape[1] for i in (2, 6, 7, 8))
    heads = query // NOPE
    even = heads % n == 0 and all(w % (128 * n) == 0 for w in (conv, query, rope, low_rank))
    if even and arrays[0].shape[1] % 32 == 0 and arrays[15].shape[1] % 128 == 0:
        return split_shards(*arrays)
    return general_shards(*arrays)


def solution(mesh):
    return jax.shard_map(
        shards if splits_well(mesh) else general_shards,
        mesh=mesh,
        in_specs=(
            P("fs", "sp", "tp"),
            P(),
            P(("sp", "fs"), "tp"),
            P(("sp", "fs"), "tp"),
            P(("sp", "fs"), "tp"),
            P(None, "tp"),
            P(("sp", "fs"), "tp"),
            P(("sp", "fs"), "tp"),
            P(("sp", "fs"), None),
            P(),
            P(),
            P(None, "tp"),
            P(None, "tp"),
            P("tp"),
            P("tp", ("sp", "fs")),
            P("tp", ("sp", "fs")),
        ),
        out_specs=P("fs", ("sp", "tp"), None),
        check_vma=False,
    )
```

```python
import functools
import math

import jax
import jax.numpy as jnp
from jax import lax
from jax.experimental import pallas as pl
from jax.experimental.pallas import tpu as pltpu
from jax.sharding import PartitionSpec as P

NOPE = 128
ROPE = 64
VD = 128
KVL = 512
SEG = 64


norm_epsilon = 1e-06
rope_theta = 10000.0


def passed_along(block, axis, distance):
    devices = range(lax.axis_size(axis))
    route = [(i - distance, i) for i in devices if i - distance in devices]
    return lax.ppermute(block, axis, route)


def rms_scale(values, gain):
    return (
        values * lax.rsqrt(jnp.mean(values * values, axis=-1, keepdims=True) + norm_epsilon) * gain
    )


def rope_tables(positions):
    half_width = ROPE // 2
    frequency = rope_theta ** (-jnp.arange(half_width, dtype=jnp.float32) * 2.0 / ROPE)
    angles = positions[:, None] * frequency[None, :]
    return (jnp.cos(angles), jnp.sin(angles))


def rotate(values, cosine, sine):
    half_width = ROPE // 2
    first = values[..., :half_width]
    second = values[..., half_width:]
    return jnp.concatenate(
        [first * cosine - second * sine, second * cosine + first * sine], axis=-1
    )


def general_shards(
    tokens,
    mix_gain,
    conv_b_weight,
    conv_c_weight,
    conv_v_weight,
    conv_taps,
    query_weight,
    query_rope_weight,
    latent_weight,
    key_rope_weight,
    latent_gain,
    key_up_weight,
    value_up_weight,
    head_gain,
    conv_out_weight,
    attn_out_weight,
):
    full_rows = lax.all_gather(tokens[0], "tp", axis=1, tiled=True)
    tok_rows = full_rows.shape[0]
    normed = rms_scale(full_rows.astype(jnp.float32), mix_gain).astype(jnp.bfloat16)
    offset = lax.axis_index("sp") * tok_rows
    token_index = offset + jnp.arange(tok_rows, dtype=jnp.int32)
    cosine, sine = rope_tables(token_index.astype(jnp.float32))
    local_heads = query_weight.shape[1] // NOPE
    count_sp = lax.axis_size("sp")
    count_fs = lax.axis_size("fs")
    count_tp = lax.axis_size("tp")
    fs_index = lax.axis_index("fs")
    row_piece = normed.shape[1] // (count_sp * count_fs)
    all_normed = lax.all_gather(normed, "fs", axis=0, tiled=True)
    picked = lax.dynamic_index_in_dim(
        all_normed.reshape(-1, count_sp, count_fs, row_piece), fs_index, 2, keepdims=False
    ).reshape(-1, count_sp * row_piece)
    gathered = (
        lax.all_gather(conv_b_weight, "sp", axis=0, tiled=True),
        lax.all_gather(conv_c_weight, "sp", axis=0, tiled=True),
        lax.all_gather(conv_v_weight, "sp", axis=0, tiled=True),
        lax.all_gather(query_weight, "sp", axis=0, tiled=True),
        lax.all_gather(query_rope_weight, "sp", axis=0, tiled=True),
        lax.all_gather(latent_weight, "sp", axis=0, tiled=True),
    )

    def project_in():
        return jnp.concatenate(
            [jnp.dot(picked, member, preferred_element_type=jnp.float32) for member in gathered],
            axis=1,
        )

    joined = lax.psum_scatter(
        project_in().astype(jnp.bfloat16), "fs", scatter_dimension=0, tiled=True
    ).astype(jnp.float32)
    bounds = []
    running_total = 0
    for member in gathered[:-1]:
        running_total = running_total + member.shape[1]
        bounds.append(running_total)
    sums = tuple(jnp.split(joined, bounds, axis=1))
    latent_raw = sums[5].astype(jnp.bfloat16)
    gate_b = sums[0].astype(jnp.bfloat16)
    gate_c = sums[1].astype(jnp.bfloat16)
    values_v = sums[2].astype(jnp.bfloat16)
    query_nope = sums[3].astype(jnp.bfloat16).reshape(tok_rows, local_heads, NOPE)
    query_rot = rotate(
        sums[4].reshape(tok_rows, local_heads, ROPE), cosine[:, None, :], sine[:, None, :]
    ).astype(jnp.bfloat16)
    latent = rms_scale(latent_raw.astype(jnp.float32), latent_gain).astype(jnp.bfloat16)
    key_rot = rotate(
        jnp.dot(normed, key_rope_weight, preferred_element_type=jnp.float32), cosine, sine
    ).astype(jnp.bfloat16)
    query_latent = jnp.einsum(
        "thn,khn->thk",
        query_nope,
        key_up_weight.reshape(KVL, local_heads, NOPE),
        preferred_element_type=jnp.float32,
    ).astype(jnp.bfloat16)
    attn_scale = (NOPE + ROPE) ** (-0.5)
    product = (gate_c.astype(jnp.float32) * values_v.astype(jnp.float32)).astype(jnp.bfloat16)
    previous = passed_along(product[tok_rows - 2 :], "sp", 1)
    padded = jnp.concatenate([previous, product], axis=0).astype(jnp.float32)
    convolved = (
        conv_taps[0] * padded[0:tok_rows]
        + conv_taps[1] * padded[1 : tok_rows + 1]
        + conv_taps[2] * padded[2 : tok_rows + 2]
    )
    conv_y = (gate_b.astype(jnp.float32) * convolved).astype(jnp.bfloat16)
    query_segment = token_index // SEG
    last_segment = (offset + tok_rows - 1) // SEG

    def key_block(running, latent_block, rot_block, first_key):
        peak_old, denom_old, accum_old = running
        block_rows = latent_block.shape[0]
        scores = (
            jnp.einsum(
                "thk,jk->thj", query_latent, latent_block, preferred_element_type=jnp.float32
            )
            + jnp.einsum("thr,jr->thj", query_rot, rot_block, preferred_element_type=jnp.float32)
        ) * attn_scale
        key_segment = (first_key + jnp.arange(block_rows, dtype=jnp.int32)) // SEG
        allowed = key_segment[None, None, :] <= query_segment[:, None, None]
        peak_new = jnp.maximum(peak_old, jnp.max(jnp.where(allowed, scores, -1e30), axis=-1))
        weights = jnp.where(allowed, jnp.exp(scores - peak_new[..., None]), 0.0)
        rescale = jnp.exp(peak_old - peak_new)
        denom_new = denom_old * rescale + jnp.sum(weights, axis=-1)
        accum_new = accum_old * rescale[..., None] + jnp.einsum(
            "thj,jk->thk",
            weights.astype(jnp.bfloat16),
            latent_block,
            preferred_element_type=jnp.float32,
        )
        return (peak_new, denom_new, accum_new)

    starting = (
        jnp.full((tok_rows, local_heads), -1e30, jnp.float32),
        jnp.zeros((tok_rows, local_heads), jnp.float32),
        jnp.zeros((tok_rows, local_heads, KVL), jnp.float32),
    )
    latent_piece = lax.all_gather(latent, "sp", axis=0, tiled=True)
    rot_piece = lax.all_gather(key_rot, "sp", axis=0, tiled=True)
    piece_rows = latent_piece.shape[0]
    splits = max(1, piece_rows // 512)
    while piece_rows % splits:
        splits = splits - 1
    block_rows = piece_rows // splits

    def visit(state, block_index):
        block_begin = block_index * block_rows
        latent_block = lax.dynamic_slice_in_dim(latent_piece, block_begin, block_rows, 0)
        rot_block = lax.dynamic_slice_in_dim(rot_piece, block_begin, block_rows, 0)
        updated = lax.cond(
            block_begin // SEG <= last_segment,
            lambda inner: key_block(inner, latent_block, rot_block, block_begin),
            lambda inner: inner,
            state,
        )
        return (updated, None)

    peak, denom, accum = lax.scan(visit, starting, jnp.arange(splits, dtype=jnp.int32))[0]
    attended = (accum / denom[..., None]).astype(jnp.bfloat16)
    head_out = jnp.einsum(
        "thk,khv->thv",
        attended,
        value_up_weight.reshape(KVL, local_heads, VD),
        preferred_element_type=jnp.float32,
    )
    normed_heads = rms_scale(head_out, head_gain.reshape(local_heads, VD))
    attn_y = normed_heads.astype(jnp.bfloat16).reshape(tok_rows, local_heads * VD)
    share_rows = tok_rows // count_tp
    conv_all, attn_all = (
        lax.all_gather(conv_y, "fs", axis=0, tiled=True),
        lax.all_gather(attn_y, "fs", axis=0, tiled=True),
    )
    conv_sorted = (
        conv_all.reshape(count_fs, count_tp, share_rows, -1)
        .transpose(1, 0, 2, 3)
        .reshape(count_fs * tok_rows, -1)
    )
    attn_sorted = (
        attn_all.reshape(count_fs, count_tp, share_rows, -1)
        .transpose(1, 0, 2, 3)
        .reshape(count_fs * tok_rows, -1)
    )
    conv_cols_sp, attn_cols_sp = (
        lax.all_gather(conv_out_weight, "sp", axis=1, tiled=True),
        lax.all_gather(attn_out_weight, "sp", axis=1, tiled=True),
    )
    col_sums = lax.psum_scatter(
        (
            jnp.dot(conv_sorted, conv_cols_sp, preferred_element_type=jnp.float32)
            + jnp.dot(attn_sorted, attn_cols_sp, preferred_element_type=jnp.float32)
        ).astype(jnp.bfloat16),
        "tp",
        scatter_dimension=0,
        tiled=True,
    )
    col_piece = conv_cols_sp.shape[1] // count_sp
    outgoing = col_sums.reshape(count_fs, share_rows, count_sp * col_piece)
    arrived = lax.all_to_all(outgoing, "fs", split_axis=0, concat_axis=2, tiled=True)
    result = (
        arrived.reshape(share_rows, count_fs, count_sp, col_piece)
        .transpose(0, 2, 1, 3)
        .reshape(share_rows, count_fs * count_sp * col_piece)
    )
    return result[None]


MESH = pl.DeviceIdType.MESH


class Place:
    def __init__(self):
        self.z = lax.axis_index("sp")
        self.f = lax.axis_index("fs")
        self.c = lax.axis_index("tp")

    def to(self, z=None, f=None, c=None):
        return {
            "sp": self.z if z is None else z,
            "fs": self.f if f is None else f,
            "tp": self.c if c is None else c,
        }


def flip(index, bit):
    digit = (index // bit) % 2
    return index + bit * (1 - 2 * digit)


def remote(src, dst, send, recv, device):
    return pltpu.make_async_remote_copy(
        src_ref=src, dst_ref=dst, send_sem=send, recv_sem=recv, device_id=device, device_id_type=MESH
    )


def greet(devices):
    barrier = pltpu.get_barrier_semaphore()
    for device in devices:
        pl.semaphore_signal(barrier, inc=1, device_id=device, device_id_type=MESH)
    pl.semaphore_wait(barrier, len(devices))


def layer_kernel(
    n,
    turns,
    tok_in,
    gain_in,
    cb,
    cc,
    cv,
    taps_in,
    qw,
    qr,
    lw,
    krw_in,
    lat_gain_in,
    key_up_in,
    value_up_in,
    head_gain_in,
    co,
    ao,
    out,
    tok,
    normed,
    win,
    wout,
    lat,
    gain,
    krw,
    taps,
    lat_gain,
    key_up,
    value_up,
    head_gain,
    conv_y,
    q_nope,
    q_rot,
    keys,
    values,
    cosine,
    sine,
    part,
    pair,
    moving,
    fetched,
    wsem,
    lsem,
    tsem,
    psem,
    latsem,
    ssem,
    pairsem,
    zsem,
):
    here = Place()
    z, f, c = here.z, here.f, here.c
    fx, fy = flip(f, 1), flip(f, 2)
    other = 1 - c
    rows = cb.shape[0]
    members = (cb, cc, cv, qw, qr, lw)
    widths = [m.shape[1] // n for m in members]
    starts = [sum(widths[:i]) for i in range(len(widths))]
    total = sum(widths)
    lat_w = widths[-1]
    proj_w = total - lat_w
    tr = tok_in.shape[1]
    length = n * tr
    half = length // 2
    outs = (co, ao)
    heights = [m.shape[0] // n for m in outs]
    tops = [sum(heights[:i]) for i in range(len(heights))]
    out_cols = co.shape[1]

    steps = [(1 + j, s) for j in range(n - 1) for s in (-1, 1)]

    greet(
        [here.to(z=lax.rem(z + j, n)) for j in range(1, n)]
        + [here.to(f=fx), here.to(f=fy), here.to(c=other)]
    )

    def in_block(zs, fs):
        return win.at[pl.ds(pl.multiple_of((zs * 4 + fs) * rows, rows), rows), :]

    def out_block(zs, fs):
        return wout.at[:, pl.ds(pl.multiple_of((zs * 4 + fs) * out_cols, out_cols), out_cols)]

    blocks = (in_block, out_block)

    def pieces(kind, dest):
        found = []
        if kind == 0:
            dst = (z * 4 + f) * rows
            for m, w, s in zip(members, widths, starts):
                src = m.at[:, pl.ds(pl.multiple_of(dest * w, w), w)]
                found.append((src, win.at[pl.ds(pl.multiple_of(dst, rows), rows), pl.ds(s, w)]))
        else:
            dst = (z * 4 + f) * out_cols
            for m, h, s in zip(outs, heights, tops):
                src = m.at[pl.ds(pl.multiple_of(dest * h, h), h), :]
                found.append((src, wout.at[pl.ds(s, h), pl.ds(pl.multiple_of(dst, out_cols), out_cols)]))
        return found

    def send_own(kind):
        for src, dst in pieces(kind, z):
            remote(src, dst, wsem.at[kind, 2, z], wsem.at[kind, 3, z], here.to(f=fx)).start()
            remote(src, dst, wsem.at[kind, 4, z], wsem.at[kind, 5, z], here.to(f=fy)).start()
            pltpu.make_async_copy(src, dst, lsem.at[kind]).start()

    def send_z(kind, distance, sign):
        dest = z + sign * distance

        @pl.when((dest >= 0) & (dest < n))
        def _():
            for src, dst in pieces(kind, dest):
                remote(src, dst, wsem.at[kind, 0, dest], wsem.at[kind, 1, z], here.to(z=dest)).start()

    def plane_copy(kind, zs, role, fs, to):
        block = blocks[kind](zs, fs)
        return remote(block, block, wsem.at[kind, role, zs], wsem.at[kind, role + 1, zs], here.to(f=to))

    def relay_z(kind, distance, sign):
        zs = z + sign * distance

        @pl.when((zs >= 0) & (zs < n))
        def _():
            block = blocks[kind](zs, f)
            remote(block, block, wsem.at[kind, 0, zs], wsem.at[kind, 1, zs], here.to(z=zs)).wait_recv()
            plane_copy(kind, zs, 2, f, fx).start()
            plane_copy(kind, zs, 4, f, fy).start()

    def relay_plane(kind, zs):
        plane_copy(kind, zs, 2, fx, fx).wait_recv()

        @pl.when(zs % 2 == 0)
        def _():
            plane_copy(kind, zs, 6, fx, fy).start()

        plane_copy(kind, zs, 4, fy, fy).wait_recv()

        @pl.when(zs % 2 == 1)
        def _():
            plane_copy(kind, zs, 6, fy, fx).start()

    def tok_block(half_index, zs):
        return tok.at[half_index, pl.ds(pl.multiple_of(zs * tr, tr), tr), :]

    def tok_copy(zs, sign, hop, src=None):
        d = (sign + 1) // 2
        block = tok_block(c, zs)
        return remote(
            block if src is None else src, block, tsem.at[d, 0, hop], tsem.at[d, 1, hop], here.to(z=z + sign)
        )

    def partner_copy(zs, owner, src=None):
        block = tok_block(owner, zs)
        return remote(block if src is None else src, block, psem.at[0, zs], psem.at[1, zs], here.to(c=other))

    own_tok = tok_in.at[0]

    def can(sign):
        return (z + sign >= 0) & (z + sign < n)

    channels = widths[0]
    heads = widths[3] // NOPE
    rot_w = widths[4]
    share = tr // 2

    def columns_of(array, width):
        return array.at[:, pl.ds(pl.multiple_of(z * width, width), width)]

    small = [
        (gain_in, gain),
        (krw_in, krw.at[0:ROPE, :]),
        (krw_in, krw.at[ROPE : 2 * ROPE, :]),
        (columns_of(taps_in, channels), taps),
        (lat_gain_in, lat_gain),
        (columns_of(key_up_in, heads * NOPE), key_up),
        (columns_of(value_up_in, heads * VD), value_up),
        (columns_of(head_gain_in, heads * VD), head_gain),
    ]

    send_own(0)
    for distance, sign in steps[:2]:
        send_z(0, distance, sign)
    partner_copy(z, c, own_tok).start()
    pltpu.make_async_copy(own_tok, tok_block(c, z), lsem.at[2]).start()
    for sign in (-1, 1):
        pl.when(can(sign))(lambda sign=sign: tok_copy(z, sign, 0, own_tok).start())
    for distance, sign in steps[2:]:
        send_z(0, distance, sign)
    for i, (src, dst) in enumerate(small):
        pltpu.make_async_copy(src, dst, ssem.at[i]).start()

    def relay_tok(distance, sign):
        zs = z + sign * distance

        @pl.when((zs >= 0) & (zs < n))
        def _():
            tok_copy(zs, -sign, distance - 1).wait_recv()
            if distance < n - 1:
                pl.when(can(-sign))(lambda: tok_copy(zs, -sign, distance).start())
            partner_copy(zs, c).start()

    def each_zs(fn):
        def body(i, carry):
            fn(lax.rem(z + i, n))
            return carry

        lax.fori_loop(0, n, body, 0)

    def at_distance(distance, fn):
        if distance == 0:
            fn(z)
            return
        for sign in (-1, 1):
            zs = z + sign * distance
            pl.when((zs >= 0) & (zs < n))(lambda zs=zs: fn(zs))

    lane = lax.broadcasted_iota(jnp.int32, (tr, rot_w), 1)
    quarter = lane % (ROPE // 2)
    first_half = (lane % ROPE) < ROPE // 2
    frequency = jnp.exp(quarter.astype(jnp.float32) * (-2.0 / ROPE * math.log(rope_theta)))

    def tables(i, carry):
        at = pl.ds(pl.multiple_of(i * tr, tr), tr)
        position = (i * tr + lax.broadcasted_iota(jnp.int32, (tr, rot_w), 0)).astype(jnp.float32)
        angle = position * frequency
        cosine[at, :] = jnp.cos(angle)
        turned = jnp.sin(angle)
        sine[at, :] = jnp.where(first_half, -turned, turned)
        return carry

    lax.fori_loop(0, n, tables, 0)

    def rotated(x, at):
        swapped = jnp.where(
            first_half, pltpu.roll(x, rot_w - ROPE // 2, 1), pltpu.roll(x, ROPE // 2, 1)
        )
        return (x * cosine[at, :] + swapped * sine[at, :]).astype(jnp.bfloat16)

    for i, (src, dst) in enumerate(small):
        pltpu.make_async_copy(src, dst, ssem.at[i]).wait()
    chunk = tr // 2
    wide = tok.shape[2]

    def norm_block(zs):
        partner_copy(zs, other).wait_recv()

        def norm_chunk(i, carry):
            at = pl.ds(pl.multiple_of(zs * tr + i * chunk, chunk), chunk)
            first = tok[0, at, :].astype(jnp.float32)
            second = tok[1, at, :].astype(jnp.float32)
            mean = (
                jnp.sum(first * first, axis=-1, keepdims=True)
                + jnp.sum(second * second, axis=-1, keepdims=True)
            ) / (2 * wide)
            scale = lax.rsqrt(mean + norm_epsilon)
            normed[at, 0:wide] = (first * scale * gain[0:1, 0:wide]).astype(jnp.bfloat16)
            normed[at, wide : 2 * wide] = (second * scale * gain[0:1, wide : 2 * wide]).astype(jnp.bfloat16)
            return carry

        lax.fori_loop(0, 2, norm_chunk, 0)

    pltpu.make_async_copy(own_tok, tok_block(c, z), lsem.at[2]).wait()
    for distance in range(1, n):
        for sign in (-1, 1):
            relay_z(0, distance, sign)
        for sign in (-1, 1):
            relay_tok(distance, sign)
        at_distance(distance - 1, lambda zs: relay_plane(0, zs))
        at_distance(distance - 1, norm_block)
    send_own(1)
    for distance, sign in steps:
        send_z(1, distance, sign)
    at_distance(n - 1, lambda zs: relay_plane(0, zs))
    at_distance(n - 1, norm_block)

    def relay_done(kind, zs):
        plane_copy(kind, zs, 6, flip(fx, 2), fx).wait_recv()

    pltpu.make_async_copy(in_block(z, f), in_block(z, f), lsem.at[0]).wait()
    each_zs(lambda zs: relay_done(0, zs))

    def lat_block(zs, owner):
        return lat.at[zs, pl.ds(pl.multiple_of(owner * half, half), half), :]

    def lat_copy(dest):
        return remote(lat_block(z, c), lat_block(z, c), latsem.at[0, dest], latsem.at[1, z], here.to(z=dest))

    def lat_arrival(zs):
        return remote(lat_block(zs, c), lat_block(zs, c), latsem.at[0, zs], latsem.at[1, zs], here.to(z=zs))

    def lat_partner(zs, owner):
        return remote(
            lat_block(zs, owner), lat_block(zs, owner), latsem.at[2, zs], latsem.at[3, zs], here.to(c=other)
        )

    mine = pl.ds(pl.multiple_of(c * half, half), half)
    lat[z, mine, :] = jnp.dot(
        normed[mine, :], win[:, proj_w:total], preferred_element_type=jnp.float32
    ).astype(jnp.bfloat16)
    for j in range(1, n):
        lat_copy(lax.rem(z + j, n)).start()
    lat_partner(z, c).start()
    for distance in range(1, n):
        for sign in (-1, 1):
            relay_z(1, distance, sign)
        at_distance(distance - 1, lambda zs: relay_plane(1, zs))

    def project(i, carry):
        at = pl.ds(pl.multiple_of(i * tr, tr), tr)
        block = normed[at, :]
        joined = jnp.dot(block, win[:, 0:proj_w], preferred_element_type=jnp.float32)
        gates = joined[:, 0 : 3 * channels].astype(jnp.bfloat16).astype(jnp.float32)
        gate_b = gates[:, 0:channels]
        product = (
            (gates[:, channels : 2 * channels] * gates[:, 2 * channels : 3 * channels])
            .astype(jnp.bfloat16)
            .astype(jnp.float32)
        )
        row = lax.broadcasted_iota(jnp.int32, (tr, channels), 0)
        older, newer = carry
        once = jnp.where(row == 0, newer, pltpu.roll(product, 1, 0))
        twice = jnp.where(row == 0, older, jnp.where(row == 1, newer, pltpu.roll(product, 2, 0)))
        convolved = taps[0:1, :] * twice + taps[1:2, :] * once + taps[2:3, :] * product
        conv_y[at, :] = (gate_b * convolved).astype(jnp.bfloat16)
        start = 3 * channels
        q_nope[at, :] = joined[:, start : start + heads * NOPE].astype(jnp.bfloat16)
        q_rot[at, :] = rotated(joined[:, start + heads * NOPE :], at)
        key_raw = lax.dot_general(
            block, krw[...], (((1,), (1,)), ((), ())), preferred_element_type=jnp.float32
        )
        key_rot = rotated(key_raw, at)
        for h in range(heads):
            keys[h, at, NOPE:] = key_rot
        return product[tr - 2 : tr - 1, :], product[tr - 1 : tr, :]

    nothing = jnp.zeros((1, channels), jnp.float32)
    lax.fori_loop(0, n, project, (nothing, nothing))
    at_distance(n - 1, lambda zs: relay_plane(1, zs))
    for j in range(1, n):
        zs = lax.rem(z + j, n)
        lat_arrival(zs).wait_recv()
        lat_partner(zs, c).start()
    each_zs(lambda zs: lat_partner(zs, other).wait_recv())

    def expand(i, carry):
        at = pl.ds(pl.multiple_of(i * tr, tr), tr)
        raw = jnp.concatenate([lat[k, at, :] for k in range(n)], axis=1).astype(jnp.float32)
        mean = jnp.mean(raw * raw, axis=-1, keepdims=True)
        low = (raw * lax.rsqrt(mean + norm_epsilon) * lat_gain[0:1, :]).astype(jnp.bfloat16)
        wide_keys = jnp.dot(low, key_up[...], preferred_element_type=jnp.float32).astype(jnp.bfloat16)
        for h in range(heads):
            keys[h, at, 0:NOPE] = wide_keys[:, h * NOPE : (h + 1) * NOPE]
        values[at, :] = jnp.dot(low, value_up[...], preferred_element_type=jnp.float32).astype(jnp.bfloat16)
        return carry

    lax.fori_loop(0, n, expand, 0)
    pltpu.make_async_copy(out_block(z, f), out_block(z, f), lsem.at[1]).wait()
    each_zs(lambda zs: relay_done(1, zs))

    shift = SEG.bit_length() - 1
    row_index = lax.broadcasted_iota(jnp.int32, (tr, length), 0)
    key_segment = jnp.right_shift(lax.broadcasted_iota(jnp.int32, (tr, length), 1), shift)
    own_lanes = lane // ROPE

    def block_output(dest):
        at = pl.ds(pl.multiple_of(dest * tr, tr), tr)
        allowed = key_segment <= jnp.right_shift(row_index + dest * tr, shift)
        outputs = [conv_y[at, :]]
        rot = q_rot[at, :]
        for h in range(heads):
            query = jnp.concatenate(
                [
                    q_nope[at, h * NOPE : (h + 1) * NOPE],
                    jnp.where(own_lanes == h, rot, jnp.zeros_like(rot)),
                ],
                axis=1,
            )
            scores = lax.dot_general(
                query, keys[h], (((1,), (1,)), ((), ())), preferred_element_type=jnp.float32
            ) * (NOPE + ROPE) ** (-0.5)
            scores = jnp.where(allowed, scores, -1e30)
            weights = jnp.exp(scores - jnp.max(scores, axis=-1, keepdims=True))
            denom = jnp.sum(weights, axis=-1, keepdims=True)
            head_out = (
                jnp.dot(
                    weights.astype(jnp.bfloat16),
                    values[:, h * VD : (h + 1) * VD],
                    preferred_element_type=jnp.float32,
                )
                / denom
            )
            mean = jnp.mean(head_out * head_out, axis=-1, keepdims=True)
            gained = head_out * lax.rsqrt(mean + norm_epsilon) * head_gain[0:1, h * VD : (h + 1) * VD]
            outputs.append(gained.astype(jnp.bfloat16))
        mixed = jnp.concatenate(outputs, axis=1)
        part[dest] = jnp.dot(mixed, wout[...], preferred_element_type=jnp.float32).astype(jnp.bfloat16)

    def part_rows(dest, core):
        return part.at[dest, pl.ds(pl.multiple_of(core * share, share), share), :]

    def pair_copy(dest):
        return remote(
            part_rows(dest, other), pair.at[dest], pairsem.at[0, dest], pairsem.at[1, dest], here.to(c=other)
        )

    def line_copy(d, dest):
        return remote(
            moving.at[dest],
            fetched.at[d, dest],
            zsem.at[d, 0, dest],
            zsem.at[d, 1, dest],
            here.to(z=z + 2 * d - 1),
        )

    def turn_of(t):
        dest = jnp.int32(0)
        for zz in range(n):
            for tt in range(n):
                dest = jnp.where((z == zz) & (t == tt), turns[zz][tt], dest)
        return dest

    def summed(dest):
        kept = part[dest, pl.ds(pl.multiple_of(c * share, share), share), :]
        return kept.astype(jnp.float32) + pair[dest].astype(jnp.float32)

    def pass_on(dest):
        d = jnp.where(dest > z, 1, 0)
        before = z - (2 * d - 1)
        has = (before >= 0) & (before < n)
        pair_copy(dest).wait_recv()

        @pl.when(has)
        def _():
            line_copy(d, dest).wait_recv()
            moving[dest] = (summed(dest) + fetched[d, dest].astype(jnp.float32)).astype(jnp.bfloat16)

        @pl.when(jnp.logical_not(has))
        def _():
            moving[dest] = summed(dest).astype(jnp.bfloat16)

        line_copy(d, dest).start()

    def turn(t, carry):
        dest = turn_of(t)
        block_output(dest)
        pair_copy(dest).start()
        pl.when(t >= 1)(lambda: pass_on(turn_of(t - 1)))
        return carry

    lax.fori_loop(0, n, turn, 0)
    pair_copy(z).wait_recv()
    low, high = z > 0, z < n - 1

    @pl.when(low)
    def _():
        line_copy(1, z).wait_recv()

    @pl.when(high)
    def _():
        line_copy(0, z).wait_recv()

    @pl.when(low & high)
    def _():
        out[...] = (
            summed(z) + fetched[1, z].astype(jnp.float32) + fetched[0, z].astype(jnp.float32)
        ).astype(jnp.bfloat16)

    @pl.when(jnp.logical_not(low & high))
    def _():
        d = jnp.where(low, 1, 0)
        out[...] = (summed(z) + fetched[d, z].astype(jnp.float32)).astype(jnp.bfloat16)

    for j in range(1, n):
        zs = lax.rem(z + j, n)
        for kind in (0, 1):
            block = blocks[kind](zs, f)
            remote(block, block, wsem.at[kind, 0, zs], wsem.at[kind, 1, zs], here.to(z=zs)).wait_send()
        lat_copy(zs).wait_send()
        line_copy(jnp.where(zs > z, 1, 0), zs).wait_send()

    def sent(zs):
        for kind in (0, 1):
            plane_copy(kind, zs, 2, f, fx).wait_send()
            plane_copy(kind, zs, 4, f, fy).wait_send()
            plane_copy(kind, zs, 6, fx, fy).wait_send()
        partner_copy(zs, c).wait_send()
        lat_partner(zs, c).wait_send()
        pair_copy(zs).wait_send()

    each_zs(sent)
    for sign in (-1, 1):
        pl.when(can(sign))(lambda sign=sign: tok_copy(z, sign, 0).wait_send())
        for distance in range(1, n - 1):
            zs = z - sign * distance
            pl.when((zs >= 0) & (zs < n) & can(sign))(
                lambda sign=sign, distance=distance: tok_copy(z, sign, distance).wait_send()
            )


def split_shards(
    tokens,
    mix_gain,
    conv_b_weight,
    conv_c_weight,
    conv_v_weight,
    conv_taps,
    query_weight,
    query_rope_weight,
    latent_weight,
    key_rope_weight,
    latent_gain,
    key_up_weight,
    value_up_weight,
    head_gain,
    conv_out_weight,
    attn_out_weight,
):
    n = lax.axis_size("sp")
    tr = tokens.shape[1]
    wide = tokens.shape[2]
    length = n * tr
    features = 2 * wide
    heads = query_weight.shape[1] // NOPE // n
    channels = conv_b_weight.shape[1] // n
    lat_w = latent_weight.shape[1] // n
    proj_w = 3 * channels + heads * (NOPE + ROPE)
    out_rows = (conv_out_weight.shape[0] + attn_out_weight.shape[0]) // n
    columns = attn_out_weight.shape[1] * n * 4
    share = tr // 2
    bf16, f32 = jnp.bfloat16, jnp.float32
    turns = [sorted(range(n), key=lambda dest: (-abs(dest - at), dest)) for at in range(n)]
    dma = pltpu.SemaphoreType.DMA
    result = pl.pallas_call(
        functools.partial(layer_kernel, n, turns),
        out_shape=jax.ShapeDtypeStruct((share, columns), bf16),
        in_specs=[pl.BlockSpec(memory_space=pltpu.HBM)] * 16,
        out_specs=pl.BlockSpec(memory_space=pltpu.VMEM),
        scratch_shapes=[
            pltpu.VMEM((2, length, wide), bf16),
            pltpu.VMEM((length, features), bf16),
            pltpu.VMEM((features, proj_w + lat_w), bf16),
            pltpu.VMEM((out_rows, columns), bf16),
            pltpu.VMEM((n, length, lat_w), bf16),
            pltpu.VMEM((8, features), f32),
            pltpu.VMEM((2 * ROPE, features), bf16),
            pltpu.VMEM((8, channels), f32),
            pltpu.VMEM((8, n * lat_w), f32),
            pltpu.VMEM((n * lat_w, heads * NOPE), bf16),
            pltpu.VMEM((n * lat_w, heads * VD), bf16),
            pltpu.VMEM((8, heads * VD), f32),
            pltpu.VMEM((length, channels), bf16),
            pltpu.VMEM((length, heads * NOPE), bf16),
            pltpu.VMEM((length, heads * ROPE), bf16),
            pltpu.VMEM((heads, length, NOPE + 2 * ROPE), bf16),
            pltpu.VMEM((length, heads * VD), bf16),
            pltpu.VMEM((length, heads * ROPE), f32),
            pltpu.VMEM((length, heads * ROPE), f32),
            pltpu.VMEM((n, tr, columns), bf16),
            pltpu.VMEM((n, share, columns), bf16),
            pltpu.VMEM((n, share, columns), bf16),
            pltpu.VMEM((2, n, share, columns), bf16),
            dma((2, 8, n)),
            dma((3,)),
            dma((2, 2, n)),
            dma((2, n)),
            dma((4, n)),
            dma((8,)),
            dma((2, n)),
            dma((2, 2, n)),
        ],
        compiler_params=pltpu.CompilerParams(
            collective_id=0, has_side_effects=True, vmem_limit_bytes=56 * 1024 * 1024
        ),
        name="whole_layer",
    )(
        tokens,
        jnp.broadcast_to(mix_gain, (8, features)),
        conv_b_weight,
        conv_c_weight,
        conv_v_weight,
        jnp.concatenate([conv_taps, jnp.zeros((8 - conv_taps.shape[0], conv_taps.shape[1]), f32)], axis=0),
        query_weight,
        query_rope_weight,
        latent_weight,
        key_rope_weight.T,
        jnp.broadcast_to(latent_gain, (8, n * lat_w)),
        key_up_weight,
        value_up_weight,
        jnp.broadcast_to(head_gain, (8, head_gain.shape[0])),
        conv_out_weight,
        attn_out_weight,
    )
    return result[None]


def splits_well(mesh):
    n = mesh.shape["sp"]
    return n > 2 and n <= 4 and mesh.shape["fs"] == 4 and mesh.shape["tp"] == 2


def shards(*arrays):
    n = lax.axis_size("sp")
    conv, query, rope, low_rank = (arrays[i].shape[1] for i in (2, 6, 7, 8))
    heads = query // NOPE
    even = heads == n * 128 // ROPE and all(w % (128 * n) == 0 for w in (conv, query, rope, low_rank))
    if even and arrays[0].shape[1] % 32 == 0 and arrays[15].shape[1] % 128 == 0:
        return split_shards(*arrays)
    return general_shards(*arrays)


def solution(mesh):
    return jax.shard_map(
        shards if splits_well(mesh) else general_shards,
        mesh=mesh,
        in_specs=(
            P("fs", "sp", "tp"),
            P(),
            P(("sp", "fs"), "tp"),
            P(("sp", "fs"), "tp"),
            P(("sp", "fs"), "tp"),
            P(None, "tp"),
            P(("sp", "fs"), "tp"),
            P(("sp", "fs"), "tp"),
            P(("sp", "fs"), None),
            P(),
            P(),
            P(None, "tp"),
            P(None, "tp"),
            P("tp"),
            P("tp", ("sp", "fs")),
            P("tp", ("sp", "fs")),
        ),
        out_specs=P("fs", ("sp", "tp"), None),
        check_vma=False,
    )
```

```python
import functools
import math

import jax
import jax.numpy as jnp
from jax import lax
from jax.experimental import pallas as pl
from jax.experimental.pallas import tpu as pltpu
from jax.sharding import PartitionSpec as P

NOPE = 128
ROPE = 64
VD = 128
KVL = 512
SEG = 64


norm_epsilon = 1e-06
rope_theta = 10000.0


def passed_along(block, axis, distance):
    devices = range(lax.axis_size(axis))
    route = [(i - distance, i) for i in devices if i - distance in devices]
    return lax.ppermute(block, axis, route)


def rms_scale(values, gain):
    return (
        values * lax.rsqrt(jnp.mean(values * values, axis=-1, keepdims=True) + norm_epsilon) * gain
    )


def rope_tables(positions):
    half_width = ROPE // 2
    frequency = rope_theta ** (-jnp.arange(half_width, dtype=jnp.float32) * 2.0 / ROPE)
    angles = positions[:, None] * frequency[None, :]
    return (jnp.cos(angles), jnp.sin(angles))


def rotate(values, cosine, sine):
    half_width = ROPE // 2
    first = values[..., :half_width]
    second = values[..., half_width:]
    return jnp.concatenate(
        [first * cosine - second * sine, second * cosine + first * sine], axis=-1
    )


def general_shards(
    tokens,
    mix_gain,
    conv_b_weight,
    conv_c_weight,
    conv_v_weight,
    conv_taps,
    query_weight,
    query_rope_weight,
    latent_weight,
    key_rope_weight,
    latent_gain,
    key_up_weight,
    value_up_weight,
    head_gain,
    conv_out_weight,
    attn_out_weight,
):
    full_rows = lax.all_gather(tokens[0], "tp", axis=1, tiled=True)
    tok_rows = full_rows.shape[0]
    normed = rms_scale(full_rows.astype(jnp.float32), mix_gain).astype(jnp.bfloat16)
    offset = lax.axis_index("sp") * tok_rows
    token_index = offset + jnp.arange(tok_rows, dtype=jnp.int32)
    cosine, sine = rope_tables(token_index.astype(jnp.float32))
    local_heads = query_weight.shape[1] // NOPE
    count_sp = lax.axis_size("sp")
    count_fs = lax.axis_size("fs")
    count_tp = lax.axis_size("tp")
    fs_index = lax.axis_index("fs")
    row_piece = normed.shape[1] // (count_sp * count_fs)
    all_normed = lax.all_gather(normed, "fs", axis=0, tiled=True)
    picked = lax.dynamic_index_in_dim(
        all_normed.reshape(-1, count_sp, count_fs, row_piece), fs_index, 2, keepdims=False
    ).reshape(-1, count_sp * row_piece)
    gathered = (
        lax.all_gather(conv_b_weight, "sp", axis=0, tiled=True),
        lax.all_gather(conv_c_weight, "sp", axis=0, tiled=True),
        lax.all_gather(conv_v_weight, "sp", axis=0, tiled=True),
        lax.all_gather(query_weight, "sp", axis=0, tiled=True),
        lax.all_gather(query_rope_weight, "sp", axis=0, tiled=True),
        lax.all_gather(latent_weight, "sp", axis=0, tiled=True),
    )

    def project_in():
        return jnp.concatenate(
            [jnp.dot(picked, member, preferred_element_type=jnp.float32) for member in gathered],
            axis=1,
        )

    joined = lax.psum_scatter(
        project_in().astype(jnp.bfloat16), "fs", scatter_dimension=0, tiled=True
    ).astype(jnp.float32)
    bounds = []
    running_total = 0
    for member in gathered[:-1]:
        running_total = running_total + member.shape[1]
        bounds.append(running_total)
    sums = tuple(jnp.split(joined, bounds, axis=1))
    latent_raw = sums[5].astype(jnp.bfloat16)
    gate_b = sums[0].astype(jnp.bfloat16)
    gate_c = sums[1].astype(jnp.bfloat16)
    values_v = sums[2].astype(jnp.bfloat16)
    query_nope = sums[3].astype(jnp.bfloat16).reshape(tok_rows, local_heads, NOPE)
    query_rot = rotate(
        sums[4].reshape(tok_rows, local_heads, ROPE), cosine[:, None, :], sine[:, None, :]
    ).astype(jnp.bfloat16)
    latent = rms_scale(latent_raw.astype(jnp.float32), latent_gain).astype(jnp.bfloat16)
    key_rot = rotate(
        jnp.dot(normed, key_rope_weight, preferred_element_type=jnp.float32), cosine, sine
    ).astype(jnp.bfloat16)
    query_latent = jnp.einsum(
        "thn,khn->thk",
        query_nope,
        key_up_weight.reshape(KVL, local_heads, NOPE),
        preferred_element_type=jnp.float32,
    ).astype(jnp.bfloat16)
    attn_scale = (NOPE + ROPE) ** (-0.5)
    product = (gate_c.astype(jnp.float32) * values_v.astype(jnp.float32)).astype(jnp.bfloat16)
    previous = passed_along(product[tok_rows - 2 :], "sp", 1)
    padded = jnp.concatenate([previous, product], axis=0).astype(jnp.float32)
    convolved = (
        conv_taps[0] * padded[0:tok_rows]
        + conv_taps[1] * padded[1 : tok_rows + 1]
        + conv_taps[2] * padded[2 : tok_rows + 2]
    )
    conv_y = (gate_b.astype(jnp.float32) * convolved).astype(jnp.bfloat16)
    query_segment = token_index // SEG
    last_segment = (offset + tok_rows - 1) // SEG

    def key_block(running, latent_block, rot_block, first_key):
        peak_old, denom_old, accum_old = running
        block_rows = latent_block.shape[0]
        scores = (
            jnp.einsum(
                "thk,jk->thj", query_latent, latent_block, preferred_element_type=jnp.float32
            )
            + jnp.einsum("thr,jr->thj", query_rot, rot_block, preferred_element_type=jnp.float32)
        ) * attn_scale
        key_segment = (first_key + jnp.arange(block_rows, dtype=jnp.int32)) // SEG
        allowed = key_segment[None, None, :] <= query_segment[:, None, None]
        peak_new = jnp.maximum(peak_old, jnp.max(jnp.where(allowed, scores, -1e30), axis=-1))
        weights = jnp.where(allowed, jnp.exp(scores - peak_new[..., None]), 0.0)
        rescale = jnp.exp(peak_old - peak_new)
        denom_new = denom_old * rescale + jnp.sum(weights, axis=-1)
        accum_new = accum_old * rescale[..., None] + jnp.einsum(
            "thj,jk->thk",
            weights.astype(jnp.bfloat16),
            latent_block,
            preferred_element_type=jnp.float32,
        )
        return (peak_new, denom_new, accum_new)

    starting = (
        jnp.full((tok_rows, local_heads), -1e30, jnp.float32),
        jnp.zeros((tok_rows, local_heads), jnp.float32),
        jnp.zeros((tok_rows, local_heads, KVL), jnp.float32),
    )
    latent_piece = lax.all_gather(latent, "sp", axis=0, tiled=True)
    rot_piece = lax.all_gather(key_rot, "sp", axis=0, tiled=True)
    piece_rows = latent_piece.shape[0]
    splits = max(1, piece_rows // 512)
    while piece_rows % splits:
        splits = splits - 1
    block_rows = piece_rows // splits

    def visit(state, block_index):
        block_begin = block_index * block_rows
        latent_block = lax.dynamic_slice_in_dim(latent_piece, block_begin, block_rows, 0)
        rot_block = lax.dynamic_slice_in_dim(rot_piece, block_begin, block_rows, 0)
        updated = lax.cond(
            block_begin // SEG <= last_segment,
            lambda inner: key_block(inner, latent_block, rot_block, block_begin),
            lambda inner: inner,
            state,
        )
        return (updated, None)

    peak, denom, accum = lax.scan(visit, starting, jnp.arange(splits, dtype=jnp.int32))[0]
    attended = (accum / denom[..., None]).astype(jnp.bfloat16)
    head_out = jnp.einsum(
        "thk,khv->thv",
        attended,
        value_up_weight.reshape(KVL, local_heads, VD),
        preferred_element_type=jnp.float32,
    )
    normed_heads = rms_scale(head_out, head_gain.reshape(local_heads, VD))
    attn_y = normed_heads.astype(jnp.bfloat16).reshape(tok_rows, local_heads * VD)
    share_rows = tok_rows // count_tp
    conv_all, attn_all = (
        lax.all_gather(conv_y, "fs", axis=0, tiled=True),
        lax.all_gather(attn_y, "fs", axis=0, tiled=True),
    )
    conv_sorted = (
        conv_all.reshape(count_fs, count_tp, share_rows, -1)
        .transpose(1, 0, 2, 3)
        .reshape(count_fs * tok_rows, -1)
    )
    attn_sorted = (
        attn_all.reshape(count_fs, count_tp, share_rows, -1)
        .transpose(1, 0, 2, 3)
        .reshape(count_fs * tok_rows, -1)
    )
    conv_cols_sp, attn_cols_sp = (
        lax.all_gather(conv_out_weight, "sp", axis=1, tiled=True),
        lax.all_gather(attn_out_weight, "sp", axis=1, tiled=True),
    )
    col_sums = lax.psum_scatter(
        (
            jnp.dot(conv_sorted, conv_cols_sp, preferred_element_type=jnp.float32)
            + jnp.dot(attn_sorted, attn_cols_sp, preferred_element_type=jnp.float32)
        ).astype(jnp.bfloat16),
        "tp",
        scatter_dimension=0,
        tiled=True,
    )
    col_piece = conv_cols_sp.shape[1] // count_sp
    outgoing = col_sums.reshape(count_fs, share_rows, count_sp * col_piece)
    arrived = lax.all_to_all(outgoing, "fs", split_axis=0, concat_axis=2, tiled=True)
    result = (
        arrived.reshape(share_rows, count_fs, count_sp, col_piece)
        .transpose(0, 2, 1, 3)
        .reshape(share_rows, count_fs * count_sp * col_piece)
    )
    return result[None]


MESH = pl.DeviceIdType.MESH


class Place:
    def __init__(self):
        self.z = lax.axis_index("sp")
        self.f = lax.axis_index("fs")
        self.c = lax.axis_index("tp")

    def to(self, z=None, f=None, c=None):
        return {
            "sp": self.z if z is None else z,
            "fs": self.f if f is None else f,
            "tp": self.c if c is None else c,
        }


def flip(index, bit):
    digit = (index // bit) % 2
    return index + bit * (1 - 2 * digit)


def remote(src, dst, send, recv, device):
    return pltpu.make_async_remote_copy(
        src_ref=src, dst_ref=dst, send_sem=send, recv_sem=recv, device_id=device, device_id_type=MESH
    )


def greet(devices):
    barrier = pltpu.get_barrier_semaphore()
    for device in devices:
        pl.semaphore_signal(barrier, inc=1, device_id=device, device_id_type=MESH)
    pl.semaphore_wait(barrier, len(devices))


def layer_kernel(
    n,
    turns,
    tok_in,
    params,
    cb,
    cc,
    cv,
    qw,
    qr,
    lw,
    krw_in,
    key_up_in,
    value_up_in,
    co,
    ao,
    out,
    tok,
    normed,
    win,
    wout,
    lat,
    gain,
    krw,
    taps,
    lat_gain,
    key_up,
    value_up,
    head_gain,
    conv_y,
    q_nope,
    q_rot,
    keys,
    values,
    cosine,
    sine,
    part,
    pair,
    moving,
    fetched,
    wsem,
    lsem,
    tsem,
    psem,
    latsem,
    ssem,
    pairsem,
    zsem,
):
    here = Place()
    z, f, c = here.z, here.f, here.c
    fx, fy = flip(f, 1), flip(f, 2)
    other = 1 - c
    rows = cb.shape[0]
    members = (cb, cc, cv, qw, qr, lw)
    widths = [m.shape[1] // n for m in members]
    starts = [sum(widths[:i]) for i in range(len(widths))]
    total = sum(widths)
    lat_w = widths[-1]
    proj_w = total - lat_w
    tr = tok_in.shape[1]
    length = n * tr
    half = length // 2
    outs = (co, ao)
    heights = [m.shape[0] // n for m in outs]
    tops = [sum(heights[:i]) for i in range(len(heights))]
    out_cols = co.shape[1]

    steps = [(1 + j, s) for j in range(n - 1) for s in (-1, 1)]

    greet(
        [here.to(z=lax.rem(z + j, n)) for j in range(1, n)]
        + [here.to(f=fx), here.to(f=fy), here.to(c=other)]
    )

    def in_block(zs, fs):
        return win.at[pl.ds(pl.multiple_of((zs * 4 + fs) * rows, rows), rows), :]

    def out_block(zs, fs):
        return wout.at[:, pl.ds(pl.multiple_of((zs * 4 + fs) * out_cols, out_cols), out_cols)]

    blocks = (in_block, out_block)

    def pieces(kind, dest):
        found = []
        if kind == 0:
            dst = (z * 4 + f) * rows
            for m, w, s in zip(members, widths, starts):
                src = m.at[:, pl.ds(pl.multiple_of(dest * w, w), w)]
                found.append((src, win.at[pl.ds(pl.multiple_of(dst, rows), rows), pl.ds(s, w)]))
        else:
            dst = (z * 4 + f) * out_cols
            for m, h, s in zip(outs, heights, tops):
                src = m.at[pl.ds(pl.multiple_of(dest * h, h), h), :]
                found.append((src, wout.at[pl.ds(s, h), pl.ds(pl.multiple_of(dst, out_cols), out_cols)]))
        return found

    def send_own(kind):
        for src, dst in pieces(kind, z):
            remote(src, dst, wsem.at[kind, 2, z], wsem.at[kind, 3, z], here.to(f=fx)).start()
            remote(src, dst, wsem.at[kind, 4, z], wsem.at[kind, 5, z], here.to(f=fy)).start()
            pltpu.make_async_copy(src, dst, lsem.at[kind]).start()

    def send_z(kind, distance, sign):
        dest = z + sign * distance

        @pl.when((dest >= 0) & (dest < n))
        def _():
            for src, dst in pieces(kind, dest):
                remote(src, dst, wsem.at[kind, 0, dest], wsem.at[kind, 1, z], here.to(z=dest)).start()

    def plane_copy(kind, zs, role, fs, to):
        block = blocks[kind](zs, fs)
        return remote(block, block, wsem.at[kind, role, zs], wsem.at[kind, role + 1, zs], here.to(f=to))

    def relay_z(kind, distance, sign):
        zs = z + sign * distance

        @pl.when((zs >= 0) & (zs < n))
        def _():
            block = blocks[kind](zs, f)
            remote(block, block, wsem.at[kind, 0, zs], wsem.at[kind, 1, zs], here.to(z=zs)).wait_recv()
            plane_copy(kind, zs, 2, f, fx).start()
            plane_copy(kind, zs, 4, f, fy).start()

    def relay_plane(kind, zs):
        plane_copy(kind, zs, 2, fx, fx).wait_recv()

        @pl.when(zs % 2 == 0)
        def _():
            plane_copy(kind, zs, 6, fx, fy).start()

        plane_copy(kind, zs, 4, fy, fy).wait_recv()

        @pl.when(zs % 2 == 1)
        def _():
            plane_copy(kind, zs, 6, fy, fx).start()

    def tok_block(half_index, zs):
        return tok.at[half_index, pl.ds(pl.multiple_of(zs * tr, tr), tr), :]

    def tok_copy(zs, sign, hop, src=None):
        d = (sign + 1) // 2
        block = tok_block(c, zs)
        return remote(
            block if src is None else src, block, tsem.at[d, 0, hop], tsem.at[d, 1, hop], here.to(z=z + sign)
        )

    def partner_copy(zs, owner, src=None):
        block = tok_block(owner, zs)
        return remote(block if src is None else src, block, psem.at[0, zs], psem.at[1, zs], here.to(c=other))

    own_tok = tok_in.at[0]

    def can(sign):
        return (z + sign >= 0) & (z + sign < n)

    channels = widths[0]
    heads = widths[3] // NOPE
    rot_w = widths[4]
    share = tr // 2

    def columns_of(array, width):
        return array.at[:, pl.ds(pl.multiple_of(z * width, width), width)]

    low_w = n * lat_w
    shift_by = pl.multiple_of(low_w + z * heads * VD, 128)
    small = [
        (params, gain),
        (krw_in, krw.at[0:ROPE, :]),
        (krw_in, krw.at[ROPE : 2 * ROPE, :]),
        (columns_of(params, channels), taps),
        (params.at[:, 0:low_w], lat_gain),
        (columns_of(key_up_in, heads * NOPE), key_up),
        (columns_of(value_up_in, heads * VD), value_up),
        (params.at[:, pl.ds(shift_by, heads * VD)], head_gain),
    ]

    send_own(0)
    for distance, sign in steps[:2]:
        send_z(0, distance, sign)
    partner_copy(z, c, own_tok).start()
    pltpu.make_async_copy(own_tok, tok_block(c, z), lsem.at[2]).start()
    for sign in (-1, 1):
        pl.when(can(sign))(lambda sign=sign: tok_copy(z, sign, 0, own_tok).start())
    for distance, sign in steps[2:]:
        send_z(0, distance, sign)
    for i, (src, dst) in enumerate(small):
        pltpu.make_async_copy(src, dst, ssem.at[i]).start()

    def relay_tok(distance, sign):
        zs = z + sign * distance

        @pl.when((zs >= 0) & (zs < n))
        def _():
            tok_copy(zs, -sign, distance - 1).wait_recv()
            if distance < n - 1:
                pl.when(can(-sign))(lambda: tok_copy(zs, -sign, distance).start())
            partner_copy(zs, c).start()

    def each_zs(fn):
        def body(i, carry):
            fn(lax.rem(z + i, n))
            return carry

        lax.fori_loop(0, n, body, 0)

    def at_distance(distance, fn):
        if distance == 0:
            fn(z)
            return
        for sign in (-1, 1):
            zs = z + sign * distance
            pl.when((zs >= 0) & (zs < n))(lambda zs=zs: fn(zs))

    lane = lax.broadcasted_iota(jnp.int32, (tr, rot_w), 1)
    quarter = lane % (ROPE // 2)
    first_half = (lane % ROPE) < ROPE // 2
    frequency = jnp.exp(quarter.astype(jnp.float32) * (-2.0 / ROPE * math.log(rope_theta)))

    def tables(i, carry):
        at = pl.ds(pl.multiple_of(i * tr, tr), tr)
        position = (i * tr + lax.broadcasted_iota(jnp.int32, (tr, rot_w), 0)).astype(jnp.float32)
        angle = position * frequency
        cosine[at, :] = jnp.cos(angle)
        turned = jnp.sin(angle)
        sine[at, :] = jnp.where(first_half, -turned, turned)
        return carry

    lax.fori_loop(0, n, tables, 0)

    def rotated(x, at):
        swapped = jnp.where(
            first_half, pltpu.roll(x, rot_w - ROPE // 2, 1), pltpu.roll(x, ROPE // 2, 1)
        )
        return (x * cosine[at, :] + swapped * sine[at, :]).astype(jnp.bfloat16)

    for i, (src, dst) in enumerate(small):
        pltpu.make_async_copy(src, dst, ssem.at[i]).wait()
    chunk = tr // 2
    wide = tok.shape[2]

    def norm_block(zs):
        partner_copy(zs, other).wait_recv()

        def norm_chunk(i, carry):
            at = pl.ds(pl.multiple_of(zs * tr + i * chunk, chunk), chunk)
            first = tok[0, at, :].astype(jnp.float32)
            second = tok[1, at, :].astype(jnp.float32)
            mean = (
                jnp.sum(first * first, axis=-1, keepdims=True)
                + jnp.sum(second * second, axis=-1, keepdims=True)
            ) / (2 * wide)
            scale = lax.rsqrt(mean + norm_epsilon)
            normed[at, 0:wide] = (first * scale * gain[0:1, 0:wide]).astype(jnp.bfloat16)
            normed[at, wide : 2 * wide] = (second * scale * gain[0:1, wide : 2 * wide]).astype(jnp.bfloat16)
            return carry

        lax.fori_loop(0, 2, norm_chunk, 0)

    pltpu.make_async_copy(own_tok, tok_block(c, z), lsem.at[2]).wait()
    for distance in range(1, n):
        for sign in (-1, 1):
            relay_z(0, distance, sign)
        for sign in (-1, 1):
            relay_tok(distance, sign)
        at_distance(distance - 1, lambda zs: relay_plane(0, zs))
        at_distance(distance - 1, norm_block)
    send_own(1)
    for distance, sign in steps:
        send_z(1, distance, sign)
    at_distance(n - 1, lambda zs: relay_plane(0, zs))
    at_distance(n - 1, norm_block)

    def relay_done(kind, zs):
        plane_copy(kind, zs, 6, flip(fx, 2), fx).wait_recv()

    pltpu.make_async_copy(in_block(z, f), in_block(z, f), lsem.at[0]).wait()
    each_zs(lambda zs: relay_done(0, zs))

    def lat_block(zs, owner):
        return lat.at[zs, pl.ds(pl.multiple_of(owner * half, half), half), :]

    def lat_copy(dest):
        return remote(lat_block(z, c), lat_block(z, c), latsem.at[0, dest], latsem.at[1, z], here.to(z=dest))

    def lat_arrival(zs):
        return remote(lat_block(zs, c), lat_block(zs, c), latsem.at[0, zs], latsem.at[1, zs], here.to(z=zs))

    def lat_partner(zs, owner):
        return remote(
            lat_block(zs, owner), lat_block(zs, owner), latsem.at[2, zs], latsem.at[3, zs], here.to(c=other)
        )

    mine = pl.ds(pl.multiple_of(c * half, half), half)
    lat[z, mine, :] = jnp.dot(
        normed[mine, :], win[:, proj_w:total], preferred_element_type=jnp.float32
    ).astype(jnp.bfloat16)
    for j in range(1, n):
        lat_copy(lax.rem(z + j, n)).start()
    lat_partner(z, c).start()
    for distance in range(1, n):
        for sign in (-1, 1):
            relay_z(1, distance, sign)
        at_distance(distance - 1, lambda zs: relay_plane(1, zs))

    def project(i, carry):
        at = pl.ds(pl.multiple_of(i * tr, tr), tr)
        block = normed[at, :]
        joined = jnp.dot(block, win[:, 0:proj_w], preferred_element_type=jnp.float32)
        gates = joined[:, 0 : 3 * channels].astype(jnp.bfloat16).astype(jnp.float32)
        gate_b = gates[:, 0:channels]
        product = (
            (gates[:, channels : 2 * channels] * gates[:, 2 * channels : 3 * channels])
            .astype(jnp.bfloat16)
            .astype(jnp.float32)
        )
        row = lax.broadcasted_iota(jnp.int32, (tr, channels), 0)
        older, newer = carry
        once = jnp.where(row == 0, newer, pltpu.roll(product, 1, 0))
        twice = jnp.where(row == 0, older, jnp.where(row == 1, newer, pltpu.roll(product, 2, 0)))
        convolved = taps[2:3, :] * twice + taps[3:4, :] * once + taps[4:5, :] * product
        conv_y[at, :] = (gate_b * convolved).astype(jnp.bfloat16)
        start = 3 * channels
        q_nope[at, :] = joined[:, start : start + heads * NOPE].astype(jnp.bfloat16)
        q_rot[at, :] = rotated(joined[:, start + heads * NOPE :], at)
        key_raw = lax.dot_general(
            block, krw[...], (((1,), (1,)), ((), ())), preferred_element_type=jnp.float32
        )
        key_rot = rotated(key_raw, at)
        for h in range(heads):
            keys[h, at, NOPE:] = key_rot
        return product[tr - 2 : tr - 1, :], product[tr - 1 : tr, :]

    nothing = jnp.zeros((1, channels), jnp.float32)
    lax.fori_loop(0, n, project, (nothing, nothing))
    at_distance(n - 1, lambda zs: relay_plane(1, zs))
    for j in range(1, n):
        zs = lax.rem(z + j, n)
        lat_arrival(zs).wait_recv()
        lat_partner(zs, c).start()
    each_zs(lambda zs: lat_partner(zs, other).wait_recv())

    def expand(i, carry):
        at = pl.ds(pl.multiple_of(i * tr, tr), tr)
        raw = jnp.concatenate([lat[k, at, :] for k in range(n)], axis=1).astype(jnp.float32)
        mean = jnp.mean(raw * raw, axis=-1, keepdims=True)
        low = (raw * lax.rsqrt(mean + norm_epsilon) * lat_gain[1:2, :]).astype(jnp.bfloat16)
        wide_keys = jnp.dot(low, key_up[...], preferred_element_type=jnp.float32).astype(jnp.bfloat16)
        for h in range(heads):
            keys[h, at, 0:NOPE] = wide_keys[:, h * NOPE : (h + 1) * NOPE]
        values[at, :] = jnp.dot(low, value_up[...], preferred_element_type=jnp.float32).astype(jnp.bfloat16)
        return carry

    lax.fori_loop(0, n, expand, 0)
    pltpu.make_async_copy(out_block(z, f), out_block(z, f), lsem.at[1]).wait()
    each_zs(lambda zs: relay_done(1, zs))

    shift = SEG.bit_length() - 1
    row_index = lax.broadcasted_iota(jnp.int32, (tr, length), 0)
    key_segment = jnp.right_shift(lax.broadcasted_iota(jnp.int32, (tr, length), 1), shift)
    own_lanes = lane // ROPE

    def block_output(dest):
        at = pl.ds(pl.multiple_of(dest * tr, tr), tr)
        allowed = key_segment <= jnp.right_shift(row_index + dest * tr, shift)
        outputs = [conv_y[at, :]]
        rot = q_rot[at, :]
        for h in range(heads):
            query = jnp.concatenate(
                [
                    q_nope[at, h * NOPE : (h + 1) * NOPE],
                    jnp.where(own_lanes == h, rot, jnp.zeros_like(rot)),
                ],
                axis=1,
            )
            scores = lax.dot_general(
                query, keys[h], (((1,), (1,)), ((), ())), preferred_element_type=jnp.float32
            ) * (NOPE + ROPE) ** (-0.5)
            scores = jnp.where(allowed, scores, -1e30)
            weights = jnp.exp(scores - jnp.max(scores, axis=-1, keepdims=True))
            denom = jnp.sum(weights, axis=-1, keepdims=True)
            head_out = (
                jnp.dot(
                    weights.astype(jnp.bfloat16),
                    values[:, h * VD : (h + 1) * VD],
                    preferred_element_type=jnp.float32,
                )
                / denom
            )
            mean = jnp.mean(head_out * head_out, axis=-1, keepdims=True)
            gained = head_out * lax.rsqrt(mean + norm_epsilon) * head_gain[1:2, h * VD : (h + 1) * VD]
            outputs.append(gained.astype(jnp.bfloat16))
        mixed = jnp.concatenate(outputs, axis=1)
        part[dest] = jnp.dot(mixed, wout[...], preferred_element_type=jnp.float32).astype(jnp.bfloat16)

    def part_rows(dest, core):
        return part.at[dest, pl.ds(pl.multiple_of(core * share, share), share), :]

    def pair_copy(dest):
        return remote(
            part_rows(dest, other), pair.at[dest], pairsem.at[0, dest], pairsem.at[1, dest], here.to(c=other)
        )

    def line_copy(d, dest):
        return remote(
            moving.at[dest],
            fetched.at[d, dest],
            zsem.at[d, 0, dest],
            zsem.at[d, 1, dest],
            here.to(z=z + 2 * d - 1),
        )

    def turn_of(t):
        dest = jnp.int32(0)
        for zz in range(n):
            for tt in range(n):
                dest = jnp.where((z == zz) & (t == tt), turns[zz][tt], dest)
        return dest

    def summed(dest):
        kept = part[dest, pl.ds(pl.multiple_of(c * share, share), share), :]
        return kept.astype(jnp.float32) + pair[dest].astype(jnp.float32)

    def pass_on(dest):
        d = jnp.where(dest > z, 1, 0)
        before = z - (2 * d - 1)
        has = (before >= 0) & (before < n)
        pair_copy(dest).wait_recv()

        @pl.when(has)
        def _():
            line_copy(d, dest).wait_recv()
            moving[dest] = (summed(dest) + fetched[d, dest].astype(jnp.float32)).astype(jnp.bfloat16)

        @pl.when(jnp.logical_not(has))
        def _():
            moving[dest] = summed(dest).astype(jnp.bfloat16)

        line_copy(d, dest).start()

    def turn(t, carry):
        dest = turn_of(t)
        block_output(dest)
        pair_copy(dest).start()
        pl.when(t >= 1)(lambda: pass_on(turn_of(t - 1)))
        return carry

    lax.fori_loop(0, n, turn, 0)
    pair_copy(z).wait_recv()
    low, high = z > 0, z < n - 1

    @pl.when(low)
    def _():
        line_copy(1, z).wait_recv()

    @pl.when(high)
    def _():
        line_copy(0, z).wait_recv()

    @pl.when(low & high)
    def _():
        out[...] = (
            summed(z) + fetched[1, z].astype(jnp.float32) + fetched[0, z].astype(jnp.float32)
        ).astype(jnp.bfloat16)

    @pl.when(jnp.logical_not(low & high))
    def _():
        d = jnp.where(low, 1, 0)
        out[...] = (summed(z) + fetched[d, z].astype(jnp.float32)).astype(jnp.bfloat16)

    for j in range(1, n):
        zs = lax.rem(z + j, n)
        for kind in (0, 1):
            block = blocks[kind](zs, f)
            remote(block, block, wsem.at[kind, 0, zs], wsem.at[kind, 1, zs], here.to(z=zs)).wait_send()
        lat_copy(zs).wait_send()
        line_copy(jnp.where(zs > z, 1, 0), zs).wait_send()

    def sent(zs):
        for kind in (0, 1):
            plane_copy(kind, zs, 2, f, fx).wait_send()
            plane_copy(kind, zs, 4, f, fy).wait_send()
            plane_copy(kind, zs, 6, fx, fy).wait_send()
        partner_copy(zs, c).wait_send()
        lat_partner(zs, c).wait_send()
        pair_copy(zs).wait_send()

    each_zs(sent)
    for sign in (-1, 1):
        pl.when(can(sign))(lambda sign=sign: tok_copy(z, sign, 0).wait_send())
        for distance in range(1, n - 1):
            zs = z - sign * distance
            pl.when((zs >= 0) & (zs < n) & can(sign))(
                lambda sign=sign, distance=distance: tok_copy(z, sign, distance).wait_send()
            )


def split_shards(
    tokens,
    mix_gain,
    conv_b_weight,
    conv_c_weight,
    conv_v_weight,
    conv_taps,
    query_weight,
    query_rope_weight,
    latent_weight,
    key_rope_weight,
    latent_gain,
    key_up_weight,
    value_up_weight,
    head_gain,
    conv_out_weight,
    attn_out_weight,
):
    n = lax.axis_size("sp")
    tr = tokens.shape[1]
    wide = tokens.shape[2]
    length = n * tr
    features = 2 * wide
    heads = query_weight.shape[1] // NOPE // n
    channels = conv_b_weight.shape[1] // n
    lat_w = latent_weight.shape[1] // n
    proj_w = 3 * channels + heads * (NOPE + ROPE)
    out_rows = (conv_out_weight.shape[0] + attn_out_weight.shape[0]) // n
    columns = attn_out_weight.shape[1] * n * 4
    share = tr // 2
    bf16, f32 = jnp.bfloat16, jnp.float32
    turns = [sorted(range(n), key=lambda dest: (-abs(dest - at), dest)) for at in range(n)]
    dma = pltpu.SemaphoreType.DMA

    def row(values):
        return jnp.pad(values, (0, features - values.shape[0]))[None]

    gains = row(jnp.concatenate([latent_gain, head_gain]))
    spare = 8 - 2 - conv_taps.shape[0]
    params = jnp.concatenate(
        [mix_gain[None], gains, jnp.pad(conv_taps, ((0, spare), (0, features - conv_taps.shape[1])))], axis=0
    )
    result = pl.pallas_call(
        functools.partial(layer_kernel, n, turns),
        out_shape=jax.ShapeDtypeStruct((share, columns), bf16),
        in_specs=[pl.BlockSpec(memory_space=pltpu.HBM)] * 13,
        out_specs=pl.BlockSpec(memory_space=pltpu.VMEM),
        scratch_shapes=[
            pltpu.VMEM((2, length, wide), bf16),
            pltpu.VMEM((length, features), bf16),
            pltpu.VMEM((features, proj_w + lat_w), bf16),
            pltpu.VMEM((out_rows, columns), bf16),
            pltpu.VMEM((n, length, lat_w), bf16),
            pltpu.VMEM((8, features), f32),
            pltpu.VMEM((2 * ROPE, features), bf16),
            pltpu.VMEM((8, channels), f32),
            pltpu.VMEM((8, n * lat_w), f32),
            pltpu.VMEM((n * lat_w, heads * NOPE), bf16),
            pltpu.VMEM((n * lat_w, heads * VD), bf16),
            pltpu.VMEM((8, heads * VD), f32),
            pltpu.VMEM((length, channels), bf16),
            pltpu.VMEM((length, heads * NOPE), bf16),
            pltpu.VMEM((length, heads * ROPE), bf16),
            pltpu.VMEM((heads, length, NOPE + 2 * ROPE), bf16),
            pltpu.VMEM((length, heads * VD), bf16),
            pltpu.VMEM((length, heads * ROPE), f32),
            pltpu.VMEM((length, heads * ROPE), f32),
            pltpu.VMEM((n, tr, columns), bf16),
            pltpu.VMEM((n, share, columns), bf16),
            pltpu.VMEM((n, share, columns), bf16),
            pltpu.VMEM((2, n, share, columns), bf16),
            dma((2, 8, n)),
            dma((3,)),
            dma((2, 2, n)),
            dma((2, n)),
            dma((4, n)),
            dma((8,)),
            dma((2, n)),
            dma((2, 2, n)),
        ],
        compiler_params=pltpu.CompilerParams(
            collective_id=0, has_side_effects=True, vmem_limit_bytes=56 * 1024 * 1024
        ),
        name="whole_layer",
    )(
        tokens,
        params,
        conv_b_weight,
        conv_c_weight,
        conv_v_weight,
        query_weight,
        query_rope_weight,
        latent_weight,
        key_rope_weight.T,
        key_up_weight,
        value_up_weight,
        conv_out_weight,
        attn_out_weight,
    )
    return result[None]


def splits_well(mesh):
    n = mesh.shape["sp"]
    return n > 2 and n <= 4 and mesh.shape["fs"] == 4 and mesh.shape["tp"] == 2


def shards(*arrays):
    n = lax.axis_size("sp")
    conv, query, rope, low_rank = (arrays[i].shape[1] for i in (2, 6, 7, 8))
    heads = query // NOPE
    even = heads == n * 128 // ROPE and all(w % (128 * n) == 0 for w in (conv, query, rope, low_rank))
    if even and arrays[0].shape[1] % 32 == 0 and arrays[15].shape[1] % 128 == 0:
        return split_shards(*arrays)
    return general_shards(*arrays)


def solution(mesh):
    return jax.shard_map(
        shards if splits_well(mesh) else general_shards,
        mesh=mesh,
        in_specs=(
            P("fs", "sp", "tp"),
            P(),
            P(("sp", "fs"), "tp"),
            P(("sp", "fs"), "tp"),
            P(("sp", "fs"), "tp"),
            P(None, "tp"),
            P(("sp", "fs"), "tp"),
            P(("sp", "fs"), "tp"),
            P(("sp", "fs"), None),
            P(),
            P(),
            P(None, "tp"),
            P(None, "tp"),
            P("tp"),
            P("tp", ("sp", "fs")),
            P("tp", ("sp", "fs")),
        ),
        out_specs=P("fs", ("sp", "tp"), None),
        check_vma=False,
    )
```
